32 devices in a mesh: sp: 16 (over z, y, x), tp: 2 (over core).
Axes of the slice: x: 2, y: 2, z: 4, core: 2. Of those that a mesh axis runs over, the one named last changes fastest.
Arguments:
- residual_signal: bfloat16 [4096, 2048], P('sp'), may hold values from -6 to 6
- reading_probe_preactivations: bfloat16 [4096, 1024], P('sp', 'tp'), may hold values from -6 to 6
- keep_switch_preactivations: bfloat16 [4096, 1024], P('sp', 'tp'), may hold values from -5.5 to 5.5
- written_entries: bfloat16 [4096, 1024], P('sp', 'tp'), may hold values from -6 to 6
- emission_switch_preactivations: bfloat16 [4096, 1024], P('sp', 'tp'), may hold values from -6 to 6
- additional_shrink_amount: float32 [4096, 1024], P('sp', 'tp'), may hold values from -0.7 to 0
- complement_of_floor: float32 [1024], P('tp'), may hold values from 2.4414063e-05 to 0.1
- per_group_rescaler: float32 [128], replicated, may hold values from 0.1 to 1.9
- emission_linear_map: bfloat16 [1024, 2048], P('tp'), may hold values from -0.1875 to 0.1875
- channel_layer_rescaler: float32 [2048], replicated, may hold values from 0.1 to 1.9
- expanding_linear_map: bfloat16 [2048, 8192], P('sp', 'tp'), may hold values from -0.125 to 0.125
- contracting_linear_map: bfloat16 [2048, 8192], P('sp', 'tp'), may hold values from -0.0625 to 0.0625
Outputs:
- layer_out: bfloat16 [4096, 2048], P('sp')
The draws below stay inside these ranges and needn't reach their ends.
All inputs are finite; a program needn't handle non-finite values.
Results may differ from the reference program's by a relative error of at most 0.006.
Values may be sent and summed in bfloat16 or wider, within the bound.
A program may use at most 128 MiB of HBM per device.

```python
import jax
import jax.numpy as jnp
from jax import lax

D = 2048
HEADS = 8
HEAD = 128
FF = 8192
BLOCK = 64
TOK_DEV = 256
MIX = 1024
TOKENS = 4096


def draw_complement_of_floor(key, part):
    pick_key = jax.random.fold_in(key, 11)
    fast_key = jax.random.fold_in(key, 12)
    slow_key = jax.random.fold_in(key, 13)
    share = 0.5
    quick = jax.random.bernoulli(pick_key, share, (MIX,))
    fast_gap = jnp.exp(jax.random.uniform(fast_key, (MIX,), jnp.float32, jnp.log(0.04), jnp.log(0.1)))
    slow_gap = 2.0 / TOKENS * jnp.exp(jax.random.uniform(slow_key, (MIX,), jnp.float32, jnp.log(0.05), 0.0))
    return jnp.where(quick, fast_gap, slow_gap).astype(jnp.float32)


def draw_keep_switch_preactivations(key, part):
    offset_key = jax.random.fold_in(key, 21)
    noise_key = jax.random.fold_in(key, 22)
    offsets = jax.random.uniform(offset_key, (TOKENS // TOK_DEV,), jnp.float32, -1.5, 1.5)
    shifts = jnp.repeat(offsets, TOK_DEV, total_repeat_length=TOKENS)[:, None]
    noise = jnp.clip(jax.random.normal(noise_key, (TOKENS, MIX), jnp.float32), -4.0, 4.0)
    return (noise + shifts).astype(jnp.bfloat16)


def draw_additional_shrink_amount(key, part):
    place_key = jax.random.fold_in(key, 31)
    value_key = jax.random.fold_in(key, 32)
    places = jax.random.randint(place_key, (3,), 0, TOKENS)
    rows = jnp.arange(TOKENS)
    struck = jnp.any(rows[:, None] == places[None, :], axis=1)
    values = jnp.log(jax.random.uniform(value_key, (TOKENS, MIX), jnp.float32, 0.5, 0.8))
    return jnp.where(struck[:, None], values, 0.0).astype(jnp.float32)


def steps_of(own_key, dims, shards, low, largest):
    level = 1.0
    for position, blocks in shards:
        steps = jax.random.uniform(jax.random.fold_in(jax.random.fold_in(own_key, 6), position), (blocks,), jnp.float32, low / len(shards), largest / len(shards))
        level = level * jnp.repeat(jnp.exp(steps), dims[position] // blocks).reshape((-1,) + (1,) * (len(dims) - 1 - position))
    return level


def centred(rng, shape, width, reach, shards=(), held_as=jnp.bfloat16):
    drawn = jax.random.normal(rng, shape, jnp.float32) * width
    if len(shards) > 0:
        drawn = steps_of(rng, shape, shards, -0.22, 0.18) * drawn
    return jnp.clip(drawn, min=-reach, max=reach).astype(held_as)


def setup_inputs(seed: int = 0) -> dict:
    arg_keys = jax.random.split(jax.random.key(seed), 13)
    return {
        "residual_signal": centred(arg_keys[0], (TOKENS, D), 1.0, 6.0, ((0, 16),)),
        "reading_probe_preactivations": centred(arg_keys[1], (TOKENS, MIX), 1.0, 6.0, ((0, 16), (1, 2))),
        "keep_switch_preactivations": draw_keep_switch_preactivations(jax.random.fold_in(arg_keys[12], 71), 0),
        "written_entries": centred(arg_keys[3], (TOKENS, MIX), 1.0, 6.0, ((0, 16), (1, 2))),
        "emission_switch_preactivations": centred(arg_keys[4], (TOKENS, MIX), 1.0, 6.0, ((0, 16), (1, 2))),
        "additional_shrink_amount": draw_additional_shrink_amount(jax.random.fold_in(arg_keys[12], 71), 0),
        "complement_of_floor": draw_complement_of_floor(jax.random.fold_in(arg_keys[12], 71), 0),
        "per_group_rescaler": jnp.clip(1.0 + 0.18 * jax.random.normal(arg_keys[7], (HEAD,), jnp.float32), 0.1, 1.9),
        "emission_linear_map": centred(arg_keys[8], (MIX, D), MIX ** -0.5, 0.1875, ((0, 2),)),
        "channel_layer_rescaler": jnp.clip(1.0 + 0.18 * jax.random.normal(arg_keys[9], (D,), jnp.float32), 0.1, 1.9),
        "expanding_linear_map": centred(arg_keys[10], (D, FF), D ** -0.5, 0.125, ((0, 16), (1, 2))),
        "contracting_linear_map": centred(arg_keys[11], (D, FF), FF ** -0.5, 0.0625, ((0, 16), (1, 2))),
    }


norm_eps = 1e-06
HIGH_ACCURACY = lax.Precision.HIGHEST

def block_step(state_matrix, inputs):
    query_block_rows, key_blk, logs_blk, value_block_rows = inputs
    cumulative_decay = jnp.cumsum(logs_blk, axis=1)
    carried_state = jnp.einsum('rlb,rbz->rlz', query_block_rows * jnp.exp(cumulative_decay), state_matrix, precision=HIGH_ACCURACY)
    spread = cumulative_decay[:, :, None, :] - cumulative_decay[:, None, :, :]
    places = jnp.arange(BLOCK)
    lower = places[:, None] >= places[None, :]
    decay = jnp.exp(jnp.where(lower[None, :, :, None], spread, -jnp.inf))
    scores = jnp.einsum('htk,hsk,htsk->hts', query_block_rows, key_blk, decay, precision=HIGH_ACCURACY)
    result = carried_state + jnp.einsum('hts,hsv->htv', scores, value_block_rows, precision=HIGH_ACCURACY)
    final_state = cumulative_decay[:, -1:, :]
    decayed_key_rows = key_blk * jnp.exp(final_state - cumulative_decay)
    state_matrix = jnp.exp(final_state[:, 0, :])[..., None] * state_matrix + jnp.einsum('aux,auf->axf', decayed_key_rows, value_block_rows, precision=HIGH_ACCURACY)
    return (state_matrix, result)

def reference(residual_signal, reading_probe_preactivations, keep_switch_preactivations, written_entries, emission_switch_preactivations, additional_shrink_amount, complement_of_floor, per_group_rescaler, emission_linear_map, channel_layer_rescaler, expanding_linear_map, contracting_linear_map):
    count = TOKENS // BLOCK
    query_act = jax.nn.silu(reading_probe_preactivations.astype(jnp.float32))
    logarithmic_keep_fraction = jnp.logaddexp(jnp.log1p(-complement_of_floor), jnp.log(complement_of_floor) + jax.nn.log_sigmoid(keep_switch_preactivations.astype(jnp.float32))) + additional_shrink_amount
    key_part = -jnp.expm1(logarithmic_keep_fraction)
    value_part = written_entries.astype(jnp.float32)

    def to_blocks(values):
        return values.reshape(count, BLOCK, HEADS, HEAD).transpose(0, 2, 1, 3)
    start = jnp.zeros((HEADS, HEAD, HEAD), jnp.float32)
    ignored, outputs = lax.scan(block_step, start, (to_blocks(query_act), to_blocks(key_part), to_blocks(logarithmic_keep_fraction), to_blocks(value_part)))
    recurrent_output = outputs.transpose(0, 2, 1, 3).reshape(TOKENS, HEADS, HEAD)
    scaled = recurrent_output * lax.rsqrt(lax.optimization_barrier(jnp.mean(recurrent_output * recurrent_output, axis=-1, keepdims=True)) + norm_eps) * per_group_rescaler
    gated = scaled * jax.nn.silu(emission_switch_preactivations.astype(jnp.float32)).reshape(TOKENS, HEADS, HEAD)
    mixed_heads = gated.reshape(TOKENS, MIX).astype(jnp.bfloat16)
    after_mix = residual_signal.astype(jnp.float32) + jnp.dot(mixed_heads, emission_linear_map, preferred_element_type=jnp.float32)
    normed = (after_mix * lax.rsqrt(lax.optimization_barrier(jnp.mean(after_mix * after_mix, axis=-1, keepdims=True)) + norm_eps) * channel_layer_rescaler).astype(jnp.bfloat16)
    upward = jnp.dot(normed, expanding_linear_map, preferred_element_type=jnp.float32)
    hidden = jnp.square(jax.nn.relu(upward)).astype(jnp.bfloat16)
    downward = lax.dot_general(hidden, contracting_linear_map, (((1,), (1,)), ((), ())), preferred_element_type=jnp.float32)
    return (after_mix + downward).astype(jnp.bfloat16)
```

```python
import jax
import jax.numpy as jnp
from jax import lax
from jax.sharding import PartitionSpec as P

HEAD = 128
BLOCK = 64


norm_eps = 1e-06
HIGH_ACCURACY = lax.Precision.HIGHEST


def prefix(shard, axis, combine, identity):
    peers, index = (lax.axis_size(axis), lax.axis_index(axis))
    everything = jax.tree.map(lambda part: lax.all_gather(part, axis), shard)
    start = jax.tree.map(
        lambda part, zero: jnp.broadcast_to(jnp.asarray(zero, part.dtype), part.shape),
        shard,
        identity,
    )

    def turn(k, before):
        reached = k < index
        new = combine(before, jax.tree.map(lambda part: part[k], everything))
        return jax.tree.map(lambda a, b: jnp.where(reached, a, b), new, before)

    return lax.fori_loop(0, peers, turn, start)


def block_step(state_matrix, inputs):
    query_block_rows, key_blk, logs_blk, value_block_rows = inputs
    cumulative_decay = jnp.cumsum(logs_blk, axis=1)
    carried_state = jnp.einsum(
        "rlb,rbz->rlz",
        query_block_rows * jnp.exp(cumulative_decay),
        state_matrix,
        precision=HIGH_ACCURACY,
    )
    spread = cumulative_decay[:, :, None, :] - cumulative_decay[:, None, :, :]
    places = jnp.arange(BLOCK)
    lower = places[:, None] >= places[None, :]
    decay = jnp.exp(jnp.where(lower[None, :, :, None], spread, -jnp.inf))
    scores = jnp.einsum(
        "htk,hsk,htsk->hts", query_block_rows, key_blk, decay, precision=HIGH_ACCURACY
    )
    result = carried_state + jnp.einsum(
        "hts,hsv->htv", scores, value_block_rows, precision=HIGH_ACCURACY
    )
    final_state = cumulative_decay[:, -1:, :]
    decayed_key_rows = key_blk * jnp.exp(final_state - cumulative_decay)
    state_matrix = jnp.exp(final_state[:, 0, :])[..., None] * state_matrix + jnp.einsum(
        "aux,auf->axf", decayed_key_rows, value_block_rows, precision=HIGH_ACCURACY
    )
    return (state_matrix, result)


def combine_carry(earlier, later):
    return (earlier[0] * later[0], later[0][..., None] * earlier[1] + later[1])


def grouping(peers):
    line = plane = 4 if peers % 16 == 0 else 1
    outer = peers // (line * plane)

    def index(o, l, p):
        return (o * line + l) * plane + p

    lines = [
        [index(o, l, p) for l in range(line)] for o in range(outer) for p in range(plane)
    ]
    planes = [
        [index(o, l, p) for o in range(outer) for p in range(plane)] for l in range(line)
    ]
    return line, plane, outer, lines, planes


def body(
    residual_signal,
    reading_probe_preactivations,
    keep_switch_preactivations,
    written_entries,
    emission_switch_preactivations,
    additional_shrink_amount,
    complement_of_floor,
    per_group_rescaler,
    emission_linear_map,
    channel_layer_rescaler,
    expanding_linear_map,
    contracting_linear_map,
):
    positions = reading_probe_preactivations.shape[0]
    channels = reading_probe_preactivations.shape[1]
    local_heads = channels // HEAD
    count = positions // BLOCK
    query_act = jax.nn.silu(reading_probe_preactivations.astype(jnp.float32))
    logarithmic_keep_fraction = (
        jnp.logaddexp(
            jnp.log1p(-complement_of_floor),
            jnp.log(complement_of_floor)
            + jax.nn.log_sigmoid(keep_switch_preactivations.astype(jnp.float32)),
        )
        + additional_shrink_amount
    )
    key_part = -jnp.expm1(logarithmic_keep_fraction)
    value_part = written_entries.astype(jnp.float32)

    def to_blocks(values):
        return values.reshape(count, BLOCK, local_heads, HEAD).transpose(0, 2, 1, 3)

    start = jnp.zeros((local_heads, HEAD, HEAD), jnp.float32)
    state_end, outputs = lax.scan(
        block_step,
        start,
        (
            to_blocks(query_act),
            to_blocks(key_part),
            to_blocks(logarithmic_keep_fraction),
            to_blocks(value_part),
        ),
    )
    within_block_output = outputs.transpose(0, 2, 1, 3).reshape(positions, local_heads, HEAD)
    running = jnp.cumsum(logarithmic_keep_fraction, axis=0)
    decay_total = jnp.exp(running[-1]).reshape(local_heads, HEAD)
    identity = (
        jnp.ones((local_heads, HEAD), jnp.float32),
        jnp.zeros((local_heads, HEAD, HEAD), jnp.float32),
    )
    prior_state = prefix((decay_total, state_end), "sp", combine_carry, identity)
    weighted_scores = (query_act * jnp.exp(running)).reshape(positions, local_heads, HEAD)
    recurrent_output = within_block_output + jnp.einsum(
        "pnm,nmx->pnx", weighted_scores, prior_state[1], precision=HIGH_ACCURACY
    )
    scaled = (
        recurrent_output
        * lax.rsqrt(
            jnp.mean(recurrent_output * recurrent_output, axis=-1, keepdims=True) + norm_eps
        )
        * per_group_rescaler
    )
    gated = scaled * jax.nn.silu(emission_switch_preactivations.astype(jnp.float32)).reshape(
        positions, local_heads, HEAD
    )
    mixed_heads = gated.reshape(positions, channels).astype(jnp.bfloat16)
    tp = lax.axis_size("tp")
    share = positions // tp
    all_heads = lax.all_to_all(mixed_heads, "tp", split_axis=0, concat_axis=1, tiled=True)
    full_out = lax.all_gather(emission_linear_map, "tp", axis=0, tiled=True)
    own_start = lax.axis_index("tp") * share
    own_residual = lax.dynamic_slice_in_dim(residual_signal, own_start, share, 0)
    projected = jnp.dot(all_heads, full_out, preferred_element_type=jnp.float32)
    after_mix = own_residual.astype(jnp.float32) + projected
    normed = (
        after_mix
        * lax.rsqrt(jnp.mean(after_mix * after_mix, axis=-1, keepdims=True) + norm_eps)
        * channel_layer_rescaler
    ).astype(jnp.bfloat16)
    line, plane, outer, lines, planes = grouping(lax.axis_size("sp"))
    rows = expanding_linear_map.shape[0]
    width = normed.shape[1]

    def spread(weight):
        mine = lax.all_to_all(
            weight, "sp", split_axis=1, concat_axis=0, axis_index_groups=lines, tiled=True
        )
        return lax.all_gather(mine, "sp", axis=0, axis_index_groups=planes, tiled=True)

    up_whole, down_whole = spread(expanding_linear_map), spread(contracting_linear_map)
    ordered = (
        normed.reshape(share, outer, line, plane, rows).swapaxes(2, 3).reshape(share, width)
    )
    tokens = lax.all_gather(ordered, "sp", axis=0, axis_index_groups=lines, tiled=True)
    tokens = lax.all_gather(tokens, "tp", axis=0, tiled=True)
    upward = jnp.dot(tokens, up_whole, preferred_element_type=jnp.float32)
    hidden = jnp.square(jax.nn.relu(upward)).astype(jnp.bfloat16)
    partial = lax.dot_general(
        hidden, down_whole, (((1,), (1,)), ((), ())), preferred_element_type=jnp.float32
    )
    downward = lax.psum_scatter(partial, "tp", scatter_dimension=0, tiled=True)
    downward = lax.psum_scatter(
        downward.astype(jnp.bfloat16),
        "sp",
        scatter_dimension=0,
        axis_index_groups=lines,
        tiled=True,
    )
    downward = (
        downward.reshape(share, outer, plane, line, rows).swapaxes(2, 3).reshape(share, width)
    )
    finished = (after_mix + downward.astype(jnp.float32)).astype(jnp.bfloat16)
    return lax.all_gather(finished, "tp", axis=0, tiled=True)


def solution(mesh):
    return jax.shard_map(
        body,
        mesh=mesh,
        in_specs=(
            P("sp", None),
            P("sp", "tp"),
            P("sp", "tp"),
            P("sp", "tp"),
            P("sp", "tp"),
            P("sp", "tp"),
            P("tp"),
            P(),
            P("tp", None),
            P(),
            P("sp", "tp"),
            P("sp", "tp"),
        ),
        out_specs=P("sp", None),
        check_vma=False,
    )
```

```python
import functools

import jax
import jax.numpy as jnp
from jax import lax
from jax.experimental import pallas as pl
from jax.experimental.pallas import tpu as pltpu
from jax.sharding import PartitionSpec as P

HEAD = 128
BLOCK = 64


norm_eps = 1e-06
HIGH_ACCURACY = lax.Precision.HIGHEST


def prefix(shard, axis, combine, identity):
    peers, index = (lax.axis_size(axis), lax.axis_index(axis))
    everything = jax.tree.map(lambda part: lax.all_gather(part, axis), shard)
    start = jax.tree.map(
        lambda part, zero: jnp.broadcast_to(jnp.asarray(zero, part.dtype), part.shape),
        shard,
        identity,
    )

    def turn(k, before):
        reached = k < index
        new = combine(before, jax.tree.map(lambda part: part[k], everything))
        return jax.tree.map(lambda a, b: jnp.where(reached, a, b), new, before)

    return lax.fori_loop(0, peers, turn, start)


def block_step(state_matrix, inputs):
    query_block_rows, key_blk, logs_blk, value_block_rows = inputs
    cumulative_decay = jnp.cumsum(logs_blk, axis=1)
    carried_state = jnp.einsum(
        "rlb,rbz->rlz",
        query_block_rows * jnp.exp(cumulative_decay),
        state_matrix,
        precision=HIGH_ACCURACY,
    )
    spread = cumulative_decay[:, :, None, :] - cumulative_decay[:, None, :, :]
    places = jnp.arange(BLOCK)
    lower = places[:, None] >= places[None, :]
    decay = jnp.exp(jnp.where(lower[None, :, :, None], spread, -jnp.inf))
    scores = jnp.einsum(
        "htk,hsk,htsk->hts", query_block_rows, key_blk, decay, precision=HIGH_ACCURACY
    )
    result = carried_state + jnp.einsum(
        "hts,hsv->htv", scores, value_block_rows, precision=HIGH_ACCURACY
    )
    final_state = cumulative_decay[:, -1:, :]
    decayed_key_rows = key_blk * jnp.exp(final_state - cumulative_decay)
    state_matrix = jnp.exp(final_state[:, 0, :])[..., None] * state_matrix + jnp.einsum(
        "aux,auf->axf", decayed_key_rows, value_block_rows, precision=HIGH_ACCURACY
    )
    return (state_matrix, result)


def combine_carry(earlier, later):
    return (earlier[0] * later[0], later[0][..., None] * earlier[1] + later[1])


MESH = pl.DeviceIdType.MESH
TILE = 256


def grouping(peers):
    line = plane = 4 if peers % 16 == 0 else 1
    return line, plane, peers // (line * plane)


def mixer_kernel(
    line,
    plane,
    outer,
    tp,
    normed_ref,
    after_ref,
    up_ref,
    down_ref,
    out_ref,
    up_w,
    down_w,
    tok,
    hid,
    pair_send,
    pair_recv,
    keep,
    line_send,
    line_recv,
    fin,
    s1_send,
    s1_recv,
    s2_send,
    s2_recv,
    tok_send,
    tok_recv,
    tokp_send,
    tokp_recv,
    pair_ssem,
    pair_rsem,
    line_ssem,
    line_rsem,
    fin_ssem,
    fin_rsem,
    loc_sem,
):
    quads = outer * plane
    share, width = normed_ref.shape
    rows = up_ref.shape[0]
    cols = up_w.shape[3]
    me, t = lax.axis_index("sp"), lax.axis_index("tp")
    p = lax.rem(me, plane)
    l = lax.rem(me // plane, line)
    o = me // (plane * line)
    q = o * plane + p

    def line_dev(d):
        return ((o * line + lax.rem(l + d, line)) * plane + p, t)

    def quad_dev(e):
        qq = lax.rem(q + e, quads)
        return ((qq // plane * line + l) * plane + lax.rem(qq, plane), t)

    def pair_dev(f):
        return (me, lax.rem(t + f, tp))

    barrier = pltpu.get_barrier_semaphore()
    peers = (
        [line_dev(d) for d in range(1, line)]
        + [quad_dev(e) for e in range(1, quads)]
        + [pair_dev(f) for f in range(1, tp)]
    )
    for dev in peers:
        pl.semaphore_signal(barrier, inc=1, device_id=dev, device_id_type=MESH)
    pl.semaphore_wait(barrier, len(peers))

    def remote(src, dst, ssem, rsem, dev):
        return pltpu.make_async_remote_copy(
            src_ref=src,
            dst_ref=dst,
            send_sem=ssem,
            recv_sem=rsem,
            device_id=dev,
            device_id_type=MESH,
        )

    pending = []
    mats = ((up_ref, up_w), (down_ref, down_w))

    def first_stage(m):
        src, dst = mats[m]
        copies = []
        for d in range(line):
            there = lax.rem(l + d, line)
            part = src.at[:, pl.ds(pl.multiple_of(there * cols, cols), cols)]
            if d == 0:
                copy = pltpu.make_async_copy(part, dst.at[q, l], loc_sem.at[m])
            else:
                k = m * line + d
                copy = remote(part, dst.at[q, l], s1_send.at[k], s1_recv.at[k], line_dev(d))
                pending.append(copy)
            copy.start()
            copies.append(copy)
        return copies

    def second_stage(m, copies):
        dst = mats[m][1]
        for d in range(line):
            if d == 0:
                copies[0].wait()
            else:
                copies[d].wait_recv()
            origin = lax.rem(l + line - d, line)
            for e in range(1, quads):
                k = (m * line + d) * quads + e
                copy = remote(
                    dst.at[q, origin], dst.at[q, origin], s2_send.at[k], s2_recv.at[k], quad_dev(e)
                )
                copy.start()
                arriving[m].append(copy)

    arriving = ([], [])
    own = pltpu.make_async_copy(normed_ref, tok.at[l, t], loc_sem.at[2])
    own.start()
    up_copies = first_stage(0)
    token_copies = [own]
    for d in range(1, line):
        copy = remote(normed_ref, tok.at[l, t], tok_send.at[d], tok_recv.at[d], line_dev(d))
        copy.start()
        pending.append(copy)
        token_copies.append(copy)
    down_copies = first_stage(1)
    second_stage(0, up_copies)
    second_stage(1, down_copies)
    pair_tokens = []
    for d in range(line):
        if d == 0:
            own.wait()
        else:
            token_copies[d].wait_recv()
        origin = lax.rem(l + line - d, line)
        for f in range(1, tp):
            k = d * tp + f
            copy = remote(
                tok.at[origin, t], tok.at[origin, t], tokp_send.at[k], tokp_recv.at[k], pair_dev(f)
            )
            copy.start()
            pair_tokens.append(copy)
    for copy in arriving[0]:
        copy.wait()
    for copy in pair_tokens:
        copy.wait()

    tile = min(TILE, cols)
    for block in range(line):

        @pl.loop(0, cols // tile)
        def _(n):
            at = pl.ds(pl.multiple_of(n * tile, tile), tile)
            value = jnp.dot(
                tok[block].reshape(tp * share, width),
                up_w[:, :, :, at].reshape(width, tile),
                preferred_element_type=jnp.float32,
            )
            value = jnp.maximum(value, 0.0)
            hid[block, :, at] = (value * value).astype(jnp.bfloat16)

    for copy in arriving[1]:
        copy.wait()

    def pair_copy(k, there, f):
        other = lax.rem(t + f, tp)
        i = k * tp + f
        return remote(
            pair_send.at[there, other],
            pair_recv.at[there, f],
            pair_ssem.at[i],
            pair_rsem.at[i],
            pair_dev(f),
        )

    group = width // (line * rows)
    assert group == quads

    def partial(k, there):
        @pl.loop(0, quads)
        def _(n):
            at = pl.ds(pl.multiple_of(n * line * rows, line * rows), line * rows)
            value = lax.dot_general(
                hid[there],
                down_w[n].reshape(line * rows, cols),
                (((1,), (1,)), ((), ())),
                preferred_element_type=jnp.float32,
            ).reshape(tp, share, line * rows)
            pair_send[there, :, :, at] = value.astype(jnp.bfloat16)
            for c in range(tp):

                @pl.when(t == c)
                def _():
                    keep[there, :, at] = value[c]

        for f in range(1, tp):
            pair_copy(k, there, f).start()

    def combine(k, there):
        total = keep[there]
        for f in range(1, tp):
            pair_copy(k, there, f).wait()
            total = total + pair_recv[there, f].astype(jnp.float32)
        return total

    def line_copy(k, there):
        return remote(
            line_send.at[there], line_recv.at[l], line_ssem.at[k], line_rsem.at[k], line_dev(k)
        )

    order = list(range(1, line)) + [0]
    for i, k in enumerate(order):
        partial(k, lax.rem(l + k, line))
        if i > 0:
            before = order[i - 1]
            there = lax.rem(l + before, line)
            line_send[there] = combine(before, there).astype(jnp.bfloat16)
            line_copy(before, there).start()
    total = after_ref[...] + combine(0, l)
    for k in range(1, line):
        line_copy(k, lax.rem(l + k, line)).wait()
        total = total + line_recv[lax.rem(l + line - k, line)].astype(jnp.float32)
    fin[...] = total.astype(jnp.bfloat16)
    out_ref[t] = fin[...]
    last = [
        remote(fin, out_ref.at[t], fin_ssem.at[f], fin_rsem.at[f], pair_dev(f))
        for f in range(1, tp)
    ]
    for copy in last:
        copy.start()
    for copy in last:
        copy.wait()
    for copy in pending:
        copy.wait_send()


def mixer(normed, after_mix, up, down, line, plane, outer):
    tp = lax.axis_size("tp")
    quads = outer * plane
    share, width = normed.shape
    rows, hidden = up.shape
    cols = hidden // line
    bf16, f32 = jnp.bfloat16, jnp.float32
    dma = pltpu.SemaphoreType.DMA
    return pl.pallas_call(
        functools.partial(mixer_kernel, line, plane, outer, tp),
        out_shape=jax.ShapeDtypeStruct((tp, share, width), bf16),
        in_specs=[pl.BlockSpec(memory_space=pltpu.VMEM)] * 4,
        out_specs=pl.BlockSpec(memory_space=pltpu.VMEM),
        scratch_shapes=[
            pltpu.VMEM((quads, line, rows, cols), bf16),
            pltpu.VMEM((quads, line, rows, cols), bf16),
            pltpu.VMEM((line, tp, share, width), bf16),
            pltpu.VMEM((line, tp * share, cols), bf16),
            pltpu.VMEM((line, tp, share, width), bf16),
            pltpu.VMEM((line, tp, share, width), bf16),
            pltpu.VMEM((line, share, width), f32),
            pltpu.VMEM((line, share, width), bf16),
            pltpu.VMEM((line, share, width), bf16),
            pltpu.VMEM((share, width), bf16),
            dma((2 * line,)),
            dma((2 * line,)),
            dma((2 * line * quads,)),
            dma((2 * line * quads,)),
            dma((line,)),
            dma((line,)),
            dma((line * tp,)),
            dma((line * tp,)),
            dma((line * tp,)),
            dma((line * tp,)),
            dma((line,)),
            dma((line,)),
            dma((tp,)),
            dma((tp,)),
            dma((3,)),
        ],
        compiler_params=pltpu.CompilerParams(
            collective_id=0, has_side_effects=True, vmem_limit_bytes=60 * 1024 * 1024
        ),
    )(normed, after_mix, up, down)


def body(
    residual_signal,
    reading_probe_preactivations,
    keep_switch_preactivations,
    written_entries,
    emission_switch_preactivations,
    additional_shrink_amount,
    complement_of_floor,
    per_group_rescaler,
    emission_linear_map,
    channel_layer_rescaler,
    expanding_linear_map,
    contracting_linear_map,
):
    positions = reading_probe_preactivations.shape[0]
    channels = reading_probe_preactivations.shape[1]
    local_heads = channels // HEAD
    count = positions // BLOCK
    query_act = jax.nn.silu(reading_probe_preactivations.astype(jnp.float32))
    logarithmic_keep_fraction = (
        jnp.logaddexp(
            jnp.log1p(-complement_of_floor),
            jnp.log(complement_of_floor)
            + jax.nn.log_sigmoid(keep_switch_preactivations.astype(jnp.float32)),
        )
        + additional_shrink_amount
    )
    key_part = -jnp.expm1(logarithmic_keep_fraction)
    value_part = written_entries.astype(jnp.float32)

    def to_blocks(values):
        return values.reshape(count, BLOCK, local_heads, HEAD).transpose(0, 2, 1, 3)

    start = jnp.zeros((local_heads, HEAD, HEAD), jnp.float32)
    state_end, outputs = lax.scan(
        block_step,
        start,
        (
            to_blocks(query_act),
            to_blocks(key_part),
            to_blocks(logarithmic_keep_fraction),
            to_blocks(value_part),
        ),
    )
    within_block_output = outputs.transpose(0, 2, 1, 3).reshape(positions, local_heads, HEAD)
    running = jnp.cumsum(logarithmic_keep_fraction, axis=0)
    decay_total = jnp.exp(running[-1]).reshape(local_heads, HEAD)
    identity = (
        jnp.ones((local_heads, HEAD), jnp.float32),
        jnp.zeros((local_heads, HEAD, HEAD), jnp.float32),
    )
    prior_state = prefix((decay_total, state_end), "sp", combine_carry, identity)
    weighted_scores = (query_act * jnp.exp(running)).reshape(positions, local_heads, HEAD)
    recurrent_output = within_block_output + jnp.einsum(
        "pnm,nmx->pnx", weighted_scores, prior_state[1], precision=HIGH_ACCURACY
    )
    scaled = (
        recurrent_output
        * lax.rsqrt(
            jnp.mean(recurrent_output * recurrent_output, axis=-1, keepdims=True) + norm_eps
        )
        * per_group_rescaler
    )
    gated = scaled * jax.nn.silu(emission_switch_preactivations.astype(jnp.float32)).reshape(
        positions, local_heads, HEAD
    )
    mixed_heads = gated.reshape(positions, channels).astype(jnp.bfloat16)
    tp = lax.axis_size("tp")
    share = positions // tp
    all_heads = lax.all_to_all(mixed_heads, "tp", split_axis=0, concat_axis=1, tiled=True)
    full_out = lax.all_gather(emission_linear_map, "tp", axis=0, tiled=True)
    own_start = lax.axis_index("tp") * share
    own_residual = lax.dynamic_slice_in_dim(residual_signal, own_start, share, 0)
    projected = jnp.dot(all_heads, full_out, preferred_element_type=jnp.float32)
    after_mix = own_residual.astype(jnp.float32) + projected
    normed = (
        after_mix
        * lax.rsqrt(jnp.mean(after_mix * after_mix, axis=-1, keepdims=True) + norm_eps)
        * channel_layer_rescaler
    ).astype(jnp.bfloat16)
    line, plane, outer = grouping(lax.axis_size("sp"))
    rows = expanding_linear_map.shape[0]
    width = normed.shape[1]

    def ordered(values):
        return (
            values.reshape(share, outer, line, plane, rows).swapaxes(2, 3).reshape(share, width)
        )

    finished = mixer(
        ordered(normed),
        ordered(after_mix),
        expanding_linear_map,
        contracting_linear_map,
        line,
        plane,
        outer,
    )
    return (
        finished.reshape(positions, outer, plane, line, rows)
        .swapaxes(2, 3)
        .reshape(positions, width)
    )


def solution(mesh):
    return jax.shard_map(
        body,
        mesh=mesh,
        in_specs=(
            P("sp", None),
            P("sp", "tp"),
            P("sp", "tp"),
            P("sp", "tp"),
            P("sp", "tp"),
            P("sp", "tp"),
            P("tp"),
            P(),
            P("tp", None),
            P(),
            P("sp", "tp"),
            P("sp", "tp"),
        ),
        out_specs=P("sp", None),
        check_vma=False,
    )
```

```python
import functools

import jax
import jax.numpy as jnp
from jax import lax
from jax.experimental import pallas as pl
from jax.experimental.pallas import tpu as pltpu
from jax.sharding import PartitionSpec as P

HEAD = 128
BLOCK = 64


norm_eps = 1e-06
HIGH_ACCURACY = lax.Precision.HIGHEST


def block_step(state_matrix, inputs):
    query_block_rows, key_blk, logs_blk, value_block_rows = inputs
    cumulative_decay = jnp.cumsum(logs_blk, axis=1)
    carried_state = jnp.einsum(
        "rlb,rbz->rlz",
        query_block_rows * jnp.exp(cumulative_decay),
        state_matrix,
        precision=HIGH_ACCURACY,
    )
    spread = cumulative_decay[:, :, None, :] - cumulative_decay[:, None, :, :]
    places = jnp.arange(BLOCK)
    lower = places[:, None] >= places[None, :]
    decay = jnp.exp(jnp.where(lower[None, :, :, None], spread, -jnp.inf))
    scores = jnp.einsum(
        "htk,hsk,htsk->hts", query_block_rows, key_blk, decay, precision=HIGH_ACCURACY
    )
    result = carried_state + jnp.einsum(
        "hts,hsv->htv", scores, value_block_rows, precision=HIGH_ACCURACY
    )
    final_state = cumulative_decay[:, -1:, :]
    decayed_key_rows = key_blk * jnp.exp(final_state - cumulative_decay)
    state_matrix = jnp.exp(final_state[:, 0, :])[..., None] * state_matrix + jnp.einsum(
        "aux,auf->axf", decayed_key_rows, value_block_rows, precision=HIGH_ACCURACY
    )
    return (state_matrix, result)


MESH = pl.DeviceIdType.MESH
TILE = 256


def grouping(peers):
    line = plane = 4 if peers % 16 == 0 else 1
    return line, plane, peers // (line * plane)


def mixer_kernel(
    line,
    plane,
    outer,
    tp,
    payload_ref,
    within_ref,
    query_ref,
    gate_ref,
    gain_ref,
    emission_ref,
    residual_ref,
    scale_ref,
    up_ref,
    down_ref,
    out_ref,
    gathered,
    prefixes,
    prior,
    mixed,
    heads,
    emission,
    normed,
    after,
    up_w,
    down_w,
    tok,
    hid,
    pair_send,
    pair_recv,
    keep,
    line_send,
    line_recv,
    fin,
    s1_send,
    s1_recv,
    s2_send,
    s2_recv,
    tok_send,
    tok_recv,
    tokp_send,
    tokp_recv,
    pair_ssem,
    pair_rsem,
    line_ssem,
    line_rsem,
    fin_ssem,
    fin_rsem,
    state_ssem,
    state_rsem,
    prior_ssem,
    prior_rsem,
    emis_ssem,
    emis_rsem,
    head_ssem,
    head_rsem,
    loc_sem,
):
    quads = outer * plane
    sp = quads * line
    share, width = normed.shape
    rows = up_ref.shape[0]
    cols = up_w.shape[2]
    tall = prefixes.shape[1]
    channels = emission_ref.shape[0]
    local_heads = channels // HEAD
    me, t = lax.axis_index("sp"), lax.axis_index("tp")
    p = lax.rem(me, plane)
    l = lax.rem(me // plane, line)
    o = me // (plane * line)
    q = o * plane + p

    def line_dev(d):
        return ((o * line + lax.rem(l + d, line)) * plane + p, t)

    def quad_dev(e):
        qq = lax.rem(q + e, quads)
        return ((qq // plane * line + l) * plane + lax.rem(qq, plane), t)

    def seq_dev(e):
        return (lax.rem(me + e, sp), t)

    def pair_dev(f):
        return (me, lax.rem(t + f, tp))

    barrier = pltpu.get_barrier_semaphore()
    peers = [seq_dev(e) for e in range(1, sp)] + [pair_dev(f) for f in range(1, tp)]
    for dev in peers:
        pl.semaphore_signal(barrier, inc=1, device_id=dev, device_id_type=MESH)
    pl.semaphore_wait(barrier, len(peers))

    def remote(src, dst, ssem, rsem, dev):
        return pltpu.make_async_remote_copy(
            src_ref=src,
            dst_ref=dst,
            send_sem=ssem,
            recv_sem=rsem,
            device_id=dev,
            device_id_type=MESH,
        )

    pending = []
    mats = ((up_ref, up_w), (down_ref, down_w))

    def first_stage(m):
        src, dst = mats[m]
        copies = []
        for d in range(line):
            there = lax.rem(l + d, line)
            part = src.at[:, pl.ds(pl.multiple_of(there * cols, cols), cols)]
            if d == 0:
                copy = pltpu.make_async_copy(part, dst.at[me], loc_sem.at[m])
            else:
                k = m * line + d
                copy = remote(part, dst.at[me], s1_send.at[k], s1_recv.at[k], line_dev(d))
                pending.append(copy)
            copy.start()
            copies.append(copy)
        return copies

    def second_stage(m, copies):
        dst = mats[m][1]
        for d in range(line):
            if d == 0:
                copies[0].wait()
            else:
                copies[d].wait_recv()
            origin = (o * line + lax.rem(l + line - d, line)) * plane + p
            for e in range(1, quads):
                k = (m * line + d) * quads + e
                copy = remote(
                    dst.at[origin], dst.at[origin], s2_send.at[k], s2_recv.at[k], quad_dev(e)
                )
                copy.start()
                arriving[m].append(copy)

    arriving = ([], [])

    state_copies = []
    for e in range(1, sp):
        there = lax.rem(me + e, sp)
        copy = remote(
            payload_ref.at[there], gathered.at[me], state_ssem.at[e], state_rsem.at[e], seq_dev(e)
        )
        copy.start()
        state_copies.append(copy)
    own = pltpu.make_async_copy(payload_ref.at[me], gathered.at[me], loc_sem.at[2])
    own.start()
    emis_copies = [
        pltpu.make_async_copy(emission_ref, emission.at[t], loc_sem.at[3]),
    ]
    for f in range(1, tp):
        emis_copies.append(
            remote(emission_ref, emission.at[t], emis_ssem.at[f], emis_rsem.at[f], pair_dev(f))
        )
    for copy in emis_copies:
        copy.start()
    up_copies = first_stage(0)
    own.wait()
    for copy in state_copies:
        copy.wait()
    run = jnp.zeros((tall, HEAD), jnp.float32)
    for k in range(sp):
        prefixes[k] = run
        run = gathered[k, tall : tall + 1, :] * run + gathered[k, :tall, :]
    prior_copies = []
    for e in range(1, sp):
        there = lax.rem(me + e, sp)
        copy = remote(
            prefixes.at[there], prior.at[me], prior_ssem.at[e], prior_rsem.at[e], seq_dev(e)
        )
        copy.start()
        prior_copies.append(copy)
    prior[me] = prefixes[me]
    down_copies = first_stage(1)
    second_stage(0, up_copies)
    for copy in prior_copies:
        copy.wait()
    before = prior[...].reshape(local_heads, HEAD, HEAD)
    for h in range(local_heads):
        lanes = slice(h * HEAD, (h + 1) * HEAD)
        recur = within_ref[:, lanes] + lax.dot_general(
            query_ref[:, lanes],
            before[h],
            (((1,), (1,)), ((), ())),
            precision=HIGH_ACCURACY,
            preferred_element_type=jnp.float32,
        )
        scaled = (
            recur
            * lax.rsqrt(jnp.mean(recur * recur, axis=-1, keepdims=True) + norm_eps)
            * gain_ref[...]
        )
        gated = scaled * jax.nn.silu(gate_ref[:, lanes].astype(jnp.float32))
        mixed[:, :, lanes] = gated.astype(jnp.bfloat16).reshape(tp, share, HEAD)
    head_copies = [pltpu.make_async_copy(mixed.at[t], heads.at[t], loc_sem.at[4])]
    for f in range(1, tp):
        other = lax.rem(t + f, tp)
        head_copies.append(
            remote(mixed.at[other], heads.at[t], head_ssem.at[f], head_rsem.at[f], pair_dev(f))
        )
    for copy in head_copies:
        copy.start()
    for copy in emis_copies + head_copies:
        copy.wait()
    wide = min(512, width)

    @pl.loop(0, width // wide)
    def _(n):
        at = pl.ds(pl.multiple_of(n * wide, wide), wide)
        value = residual_ref[t, :, at].astype(jnp.float32)
        for c in range(tp):
            value = value + jnp.dot(
                heads[c], emission[c, :, at], preferred_element_type=jnp.float32
            )
        after[:, at] = value

    square = jnp.mean(after[...] * after[...], axis=-1, keepdims=True)
    normed[...] = (after[...] * lax.rsqrt(square + norm_eps) * scale_ref[...]).astype(
        jnp.bfloat16
    )
    own = pltpu.make_async_copy(normed, tok.at[l, t], loc_sem.at[5])
    own.start()
    token_copies = [own]
    for d in range(1, line):
        copy = remote(normed, tok.at[l, t], tok_send.at[d], tok_recv.at[d], line_dev(d))
        copy.start()
        pending.append(copy)
        token_copies.append(copy)
    second_stage(1, down_copies)
    pair_tokens = []
    for d in range(line):
        if d == 0:
            own.wait()
        else:
            token_copies[d].wait_recv()
        origin = lax.rem(l + line - d, line)
        for f in range(1, tp):
            k = d * tp + f
            copy = remote(
                tok.at[origin, t], tok.at[origin, t], tokp_send.at[k], tokp_recv.at[k], pair_dev(f)
            )
            copy.start()
            pair_tokens.append(copy)
    for copy in arriving[0]:
        copy.wait()
    for copy in pair_tokens:
        copy.wait()

    tile = min(TILE, cols)
    for block in range(line):

        @pl.loop(0, cols // tile)
        def _(n):
            at = pl.ds(pl.multiple_of(n * tile, tile), tile)
            value = jnp.dot(
                tok[block].reshape(tp * share, width),
                up_w[:, :, at].reshape(width, tile),
                preferred_element_type=jnp.float32,
            )
            value = jnp.maximum(value, 0.0)
            hid[block, :, at] = (value * value).astype(jnp.bfloat16)

    for copy in arriving[1]:
        copy.wait()

    def pair_copy(k, there, f):
        other = lax.rem(t + f, tp)
        i = k * tp + f
        return remote(
            pair_send.at[there, other],
            pair_recv.at[there, f],
            pair_ssem.at[i],
            pair_rsem.at[i],
            pair_dev(f),
        )

    group = width // (line * rows)
    assert group == quads

    def partial(k, there):
        @pl.loop(0, quads)
        def _(n):
            at = pl.ds(pl.multiple_of(n * line * rows, line * rows), line * rows)
            value = lax.dot_general(
                hid[there],
                down_w[pl.ds(n * line, line)].reshape(line * rows, cols),
                (((1,), (1,)), ((), ())),
                preferred_element_type=jnp.float32,
            ).reshape(tp, share, line * rows)
            pair_send[there, :, :, at] = value.astype(jnp.bfloat16)
            for c in range(tp):

                @pl.when(t == c)
                def _():
                    keep[there, :, at] = value[c]

        for f in range(1, tp):
            pair_copy(k, there, f).start()

    def combine(k, there):
        total = keep[there]
        for f in range(1, tp):
            pair_copy(k, there, f).wait()
            total = total + pair_recv[there, f].astype(jnp.float32)
        return total

    def line_copy(k, there):
        return remote(
            line_send.at[there], line_recv.at[l], line_ssem.at[k], line_rsem.at[k], line_dev(k)
        )

    order = list(range(1, line)) + [0]
    for i, k in enumerate(order):
        partial(k, lax.rem(l + k, line))
        if i > 0:
            before = order[i - 1]
            there = lax.rem(l + before, line)
            line_send[there] = combine(before, there).astype(jnp.bfloat16)
            line_copy(before, there).start()
    total = after[...] + combine(0, l)
    for k in range(1, line):
        line_copy(k, lax.rem(l + k, line)).wait()
        total = total + line_recv[lax.rem(l + line - k, line)].astype(jnp.float32)
    fin[...] = total.astype(jnp.bfloat16)
    out_ref[t] = fin[...]
    last = [
        remote(fin, out_ref.at[t], fin_ssem.at[f], fin_rsem.at[f], pair_dev(f))
        for f in range(1, tp)
    ]
    for copy in last:
        copy.start()
    for copy in last:
        copy.wait()
    for copy in pending:
        copy.wait_send()


def mixer(
    payload, within, query, gate, gain, out_map, residual, scale, up, down, line, plane, outer
):
    tp = lax.axis_size("tp")
    quads = outer * plane
    sp = quads * line
    positions, width = residual.shape
    share = positions // tp
    rows, hidden = up.shape
    cols = hidden // line
    tall = payload.shape[1] - 1
    channels = within.shape[1]
    bf16, f32 = jnp.bfloat16, jnp.float32
    dma = pltpu.SemaphoreType.DMA
    return pl.pallas_call(
        functools.partial(mixer_kernel, line, plane, outer, tp),
        out_shape=jax.ShapeDtypeStruct((tp, share, width), bf16),
        in_specs=[pl.BlockSpec(memory_space=pltpu.VMEM)] * 10,
        out_specs=pl.BlockSpec(memory_space=pltpu.VMEM),
        scratch_shapes=[
            pltpu.VMEM((sp, tall + 1, HEAD), f32),
            pltpu.VMEM((sp, tall, HEAD), f32),
            pltpu.VMEM((sp, tall, HEAD), f32),
            pltpu.VMEM((tp, share, channels), bf16),
            pltpu.VMEM((tp, share, channels), bf16),
            pltpu.VMEM((tp, channels, width), bf16),
            pltpu.VMEM((share, width), bf16),
            pltpu.VMEM((share, width), f32),
            pltpu.VMEM((sp, rows, cols), bf16),
            pltpu.VMEM((sp, rows, cols), bf16),
            pltpu.VMEM((line, tp, share, width), bf16),
            pltpu.VMEM((line, tp * share, cols), bf16),
            pltpu.VMEM((line, tp, share, width), bf16),
            pltpu.VMEM((line, tp, share, width), bf16),
            pltpu.VMEM((line, share, width), f32),
            pltpu.VMEM((line, share, width), bf16),
            pltpu.VMEM((line, share, width), bf16),
            pltpu.VMEM((share, width), bf16),
            dma((2 * line,)),
            dma((2 * line,)),
            dma((2 * line * quads,)),
            dma((2 * line * quads,)),
            dma((line,)),
            dma((line,)),
            dma((line * tp,)),
            dma((line * tp,)),
            dma((line * tp,)),
            dma((line * tp,)),
            dma((line,)),
            dma((line,)),
            dma((tp,)),
            dma((tp,)),
            dma((sp,)),
            dma((sp,)),
            dma((sp,)),
            dma((sp,)),
            dma((tp,)),
            dma((tp,)),
            dma((tp,)),
            dma((tp,)),
            dma((6,)),
        ],
        compiler_params=pltpu.CompilerParams(
            collective_id=0, has_side_effects=True, vmem_limit_bytes=60 * 1024 * 1024
        ),
    )(
        payload,
        within,
        query,
        gate,
        gain.reshape(1, HEAD),
        out_map,
        residual.reshape(tp, share, width),
        scale.reshape(1, width),
        up,
        down,
    )


def body(
    residual_signal,
    reading_probe_preactivations,
    keep_switch_preactivations,
    written_entries,
    emission_switch_preactivations,
    additional_shrink_amount,
    complement_of_floor,
    per_group_rescaler,
    emission_linear_map,
    channel_layer_rescaler,
    expanding_linear_map,
    contracting_linear_map,
):
    positions = reading_probe_preactivations.shape[0]
    channels = reading_probe_preactivations.shape[1]
    local_heads = channels // HEAD
    count = positions // BLOCK
    query_act = jax.nn.silu(reading_probe_preactivations.astype(jnp.float32))
    logarithmic_keep_fraction = (
        jnp.logaddexp(
            jnp.log1p(-complement_of_floor),
            jnp.log(complement_of_floor)
            + jax.nn.log_sigmoid(keep_switch_preactivations.astype(jnp.float32)),
        )
        + additional_shrink_amount
    )
    key_part = -jnp.expm1(logarithmic_keep_fraction)
    value_part = written_entries.astype(jnp.float32)

    def to_blocks(values):
        return values.reshape(count, BLOCK, local_heads, HEAD).transpose(0, 2, 1, 3)

    start = jnp.zeros((local_heads, HEAD, HEAD), jnp.float32)
    state_end, outputs = lax.scan(
        block_step,
        start,
        (
            to_blocks(query_act),
            to_blocks(key_part),
            to_blocks(logarithmic_keep_fraction),
            to_blocks(value_part),
        ),
    )
    within_block_output = outputs.transpose(0, 2, 1, 3).reshape(positions, local_heads, HEAD)
    running = jnp.cumsum(logarithmic_keep_fraction, axis=0)
    decay_total = jnp.exp(running[-1]).reshape(local_heads, HEAD)
    sp = lax.axis_size("sp")
    tall = local_heads * HEAD // sp
    slices = state_end.swapaxes(1, 2).reshape(sp, tall, HEAD)
    fading = jnp.repeat(decay_total, sp // local_heads, axis=0).reshape(sp, 1, HEAD)
    line, plane, outer = grouping(sp)
    finished = mixer(
        jnp.concatenate([slices, fading], axis=1),
        within_block_output.reshape(positions, channels),
        query_act * jnp.exp(running),
        emission_switch_preactivations,
        per_group_rescaler,
        emission_linear_map,
        residual_signal,
        channel_layer_rescaler,
        expanding_linear_map,
        contracting_linear_map,
        line,
        plane,
        outer,
    )
    return finished.reshape(residual_signal.shape)


def solution(mesh):
    return jax.shard_map(
        body,
        mesh=mesh,
        in_specs=(
            P("sp", None),
            P("sp", "tp"),
            P("sp", "tp"),
            P("sp", "tp"),
            P("sp", "tp"),
            P("sp", "tp"),
            P("tp"),
            P(),
            P("tp", None),
            P(),
            P("sp", "tp"),
            P("sp", "tp"),
        ),
        out_specs=P("sp", None),
        check_vma=False,
    )
```

```python
import functools

import jax
import jax.numpy as jnp
from jax import lax
from jax.experimental import pallas as pl
from jax.experimental.pallas import tpu as pltpu
from jax.sharding import PartitionSpec as P

HEAD = 128
BLOCK = 64


norm_eps = 1e-06
HIGH_ACCURACY = lax.Precision.HIGHEST


MESH = pl.DeviceIdType.MESH
TILE = 256


def grouping(peers):
    line = plane = 4 if peers % 16 == 0 else 1
    return line, plane, peers // (line * plane)


def mixer_kernel(
    line,
    plane,
    outer,
    tp,
    probe_ref,
    logs_ref,
    key_ref,
    value_ref,
    gate_ref,
    gain_ref,
    emission_ref,
    residual_ref,
    scale_ref,
    up_ref,
    down_ref,
    out_ref,
    payload_ref,
    within_ref,
    query_ref,
    state,
    base,
    gathered,
    prefixes,
    prior,
    mixed,
    heads,
    emission,
    normed,
    after,
    up_w,
    down_w,
    tok,
    hid,
    pair_send,
    pair_recv,
    keep,
    line_send,
    line_recv,
    fin,
    s1_send,
    s1_recv,
    s2_send,
    s2_recv,
    tok_send,
    tok_recv,
    tokp_send,
    tokp_recv,
    pair_ssem,
    pair_rsem,
    line_ssem,
    line_rsem,
    fin_ssem,
    fin_rsem,
    state_ssem,
    state_rsem,
    prior_ssem,
    prior_rsem,
    emis_ssem,
    emis_rsem,
    head_ssem,
    head_rsem,
    loc_sem,
):
    quads = outer * plane
    sp = quads * line
    share, width = normed.shape
    rows = up_ref.shape[0]
    cols = up_w.shape[2]
    tall = prefixes.shape[1]
    channels = emission_ref.shape[0]
    local_heads = channels // HEAD
    me, t = lax.axis_index("sp"), lax.axis_index("tp")
    p = lax.rem(me, plane)
    l = lax.rem(me // plane, line)
    o = me // (plane * line)
    q = o * plane + p

    def line_dev(d):
        return ((o * line + lax.rem(l + d, line)) * plane + p, t)

    def quad_dev(e):
        qq = lax.rem(q + e, quads)
        return ((qq // plane * line + l) * plane + lax.rem(qq, plane), t)

    def seq_dev(e):
        return (lax.rem(me + e, sp), t)

    def pair_dev(f):
        return (me, lax.rem(t + f, tp))

    barrier = pltpu.get_barrier_semaphore()
    peers = [seq_dev(e) for e in range(1, sp)] + [pair_dev(f) for f in range(1, tp)]
    for dev in peers:
        pl.semaphore_signal(barrier, inc=1, device_id=dev, device_id_type=MESH)
    pl.semaphore_wait(barrier, len(peers))

    def remote(src, dst, ssem, rsem, dev):
        return pltpu.make_async_remote_copy(
            src_ref=src,
            dst_ref=dst,
            send_sem=ssem,
            recv_sem=rsem,
            device_id=dev,
            device_id_type=MESH,
        )

    pending = []
    mats = ((up_ref, up_w), (down_ref, down_w))

    def first_stage(m):
        src, dst = mats[m]
        copies = []
        for d in range(line):
            there = lax.rem(l + d, line)
            part = src.at[:, pl.ds(pl.multiple_of(there * cols, cols), cols)]
            if d == 0:
                copy = pltpu.make_async_copy(part, dst.at[me], loc_sem.at[m])
            else:
                k = m * line + d
                copy = remote(part, dst.at[me], s1_send.at[k], s1_recv.at[k], line_dev(d))
                pending.append(copy)
            copy.start()
            copies.append(copy)
        return copies

    def second_stage(m, copies):
        dst = mats[m][1]
        for d in range(line):
            if d == 0:
                copies[0].wait()
            else:
                copies[d].wait_recv()
            origin = (o * line + lax.rem(l + line - d, line)) * plane + p
            for e in range(1, quads):
                k = (m * line + d) * quads + e
                copy = remote(
                    dst.at[origin], dst.at[origin], s2_send.at[k], s2_recv.at[k], quad_dev(e)
                )
                copy.start()
                arriving[m].append(copy)

    arriving = ([], [])

    emis_copies = [
        pltpu.make_async_copy(emission_ref, emission.at[t], loc_sem.at[3]),
    ]
    for f in range(1, tp):
        emis_copies.append(
            remote(emission_ref, emission.at[t], emis_ssem.at[f], emis_rsem.at[f], pair_dev(f))
        )
    for copy in emis_copies:
        copy.start()
    up_copies = first_stage(0)
    state[...] = jnp.zeros_like(state)
    base[...] = jnp.zeros_like(base)
    lower = lax.broadcasted_iota(jnp.int32, (BLOCK, BLOCK), 0) >= lax.broadcasted_iota(
        jnp.int32, (BLOCK, BLOCK), 1
    )

    def exact(a, b, ca, cb):
        return lax.dot_general(
            a,
            b,
            (((ca,), (cb,)), ((), ())),
            precision=HIGH_ACCURACY,
            preferred_element_type=jnp.float32,
        )

    @pl.loop(0, probe_ref.shape[0] // BLOCK)
    def _(b):
        at = pl.ds(pl.multiple_of(b * BLOCK, BLOCK), BLOCK)
        sums = exact(lower.astype(jnp.float32), logs_ref[at, :], 1, 0)
        for h in range(local_heads):
            lanes = slice(h * HEAD, (h + 1) * HEAD)
            total = sums[:, lanes]
            end = total[BLOCK - 1 : BLOCK, :]
            middle = 0.5 * end
            query = jax.nn.silu(probe_ref[at, lanes].astype(jnp.float32))
            key = key_ref[at, lanes]
            value = value_ref[at, lanes].astype(jnp.float32)
            scores = exact(query * jnp.exp(total - middle), key * jnp.exp(middle - total), 1, 1)
            scores = jnp.where(lower, scores, 0.0)
            within_ref[at, lanes] = exact(scores, value, 1, 0) + exact(
                query * jnp.exp(total), state[h], 1, 1
            )
            query_ref[at, lanes] = query * jnp.exp(base[h] + total)
            state[h] = jnp.exp(end) * state[h] + exact(value, key * jnp.exp(end - total), 0, 0)
            base[h] = base[h] + end

    each = sp // local_heads
    for k in range(sp):
        h, j = divmod(k, each)
        payload_ref[k, :tall, :] = state[h, j * tall : (j + 1) * tall, :]
        payload_ref[k, tall : tall + 1, :] = jnp.exp(base[h])
    state_copies = []
    for e in range(1, sp):
        there = lax.rem(me + e, sp)
        copy = remote(
            payload_ref.at[there], gathered.at[me], state_ssem.at[e], state_rsem.at[e], seq_dev(e)
        )
        copy.start()
        state_copies.append(copy)
    own = pltpu.make_async_copy(payload_ref.at[me], gathered.at[me], loc_sem.at[2])
    own.start()
    own.wait()
    for copy in state_copies:
        copy.wait()
    run = jnp.zeros((tall, HEAD), jnp.float32)
    for k in range(sp):
        prefixes[k] = run
        run = gathered[k, tall : tall + 1, :] * run + gathered[k, :tall, :]
    prior_copies = []
    for e in range(1, sp):
        there = lax.rem(me + e, sp)
        copy = remote(
            prefixes.at[there], prior.at[me], prior_ssem.at[e], prior_rsem.at[e], seq_dev(e)
        )
        copy.start()
        prior_copies.append(copy)
    prior[me] = prefixes[me]
    down_copies = first_stage(1)
    second_stage(0, up_copies)
    for copy in prior_copies:
        copy.wait()
    before = prior[...].reshape(local_heads, HEAD, HEAD)
    for h in range(local_heads):
        lanes = slice(h * HEAD, (h + 1) * HEAD)
        recur = within_ref[:, lanes] + lax.dot_general(
            query_ref[:, lanes],
            before[h],
            (((1,), (1,)), ((), ())),
            precision=HIGH_ACCURACY,
            preferred_element_type=jnp.float32,
        )
        scaled = (
            recur
            * lax.rsqrt(jnp.mean(recur * recur, axis=-1, keepdims=True) + norm_eps)
            * gain_ref[...]
        )
        gated = scaled * jax.nn.silu(gate_ref[:, lanes].astype(jnp.float32))
        mixed[:, :, lanes] = gated.astype(jnp.bfloat16).reshape(tp, share, HEAD)
    head_copies = [pltpu.make_async_copy(mixed.at[t], heads.at[t], loc_sem.at[4])]
    for f in range(1, tp):
        other = lax.rem(t + f, tp)
        head_copies.append(
            remote(mixed.at[other], heads.at[t], head_ssem.at[f], head_rsem.at[f], pair_dev(f))
        )
    for copy in head_copies:
        copy.start()
    for copy in emis_copies + head_copies:
        copy.wait()
    wide = min(512, width)

    @pl.loop(0, width // wide)
    def _(n):
        at = pl.ds(pl.multiple_of(n * wide, wide), wide)
        value = residual_ref[t, :, at].astype(jnp.float32)
        for c in range(tp):
            value = value + jnp.dot(
                heads[c], emission[c, :, at], preferred_element_type=jnp.float32
            )
        after[:, at] = value

    square = jnp.mean(after[...] * after[...], axis=-1, keepdims=True)
    normed[...] = (after[...] * lax.rsqrt(square + norm_eps) * scale_ref[...]).astype(
        jnp.bfloat16
    )
    own = pltpu.make_async_copy(normed, tok.at[l, t], loc_sem.at[5])
    own.start()
    token_copies = [own]
    for d in range(1, line):
        copy = remote(normed, tok.at[l, t], tok_send.at[d], tok_recv.at[d], line_dev(d))
        copy.start()
        pending.append(copy)
        token_copies.append(copy)
    second_stage(1, down_copies)
    pair_tokens = []
    for d in range(line):
        if d == 0:
            own.wait()
        else:
            token_copies[d].wait_recv()
        origin = lax.rem(l + line - d, line)
        for f in range(1, tp):
            k = d * tp + f
            copy = remote(
                tok.at[origin, t], tok.at[origin, t], tokp_send.at[k], tokp_recv.at[k], pair_dev(f)
            )
            copy.start()
            pair_tokens.append(copy)
    for copy in arriving[0]:
        copy.wait()
    for copy in pair_tokens:
        copy.wait()

    tile = min(TILE, cols)
    for block in range(line):

        @pl.loop(0, cols // tile)
        def _(n):
            at = pl.ds(pl.multiple_of(n * tile, tile), tile)
            value = jnp.dot(
                tok[block].reshape(tp * share, width),
                up_w[:, :, at].reshape(width, tile),
                preferred_element_type=jnp.float32,
            )
            value = jnp.maximum(value, 0.0)
            hid[block, :, at] = (value * value).astype(jnp.bfloat16)

    for copy in arriving[1]:
        copy.wait()

    def pair_copy(k, there, f):
        other = lax.rem(t + f, tp)
        i = k * tp + f
        return remote(
            pair_send.at[there, other],
            pair_recv.at[there, f],
            pair_ssem.at[i],
            pair_rsem.at[i],
            pair_dev(f),
        )

    group = width // (line * rows)
    assert group == quads

    def partial(k, there):
        @pl.loop(0, quads)
        def _(n):
            at = pl.ds(pl.multiple_of(n * line * rows, line * rows), line * rows)
            value = lax.dot_general(
                hid[there],
                down_w[pl.ds(n * line, line)].reshape(line * rows, cols),
                (((1,), (1,)), ((), ())),
                preferred_element_type=jnp.float32,
            ).reshape(tp, share, line * rows)
            pair_send[there, :, :, at] = value.astype(jnp.bfloat16)
            for c in range(tp):

                @pl.when(t == c)
                def _():
                    keep[there, :, at] = value[c]

        for f in range(1, tp):
            pair_copy(k, there, f).start()

    def combine(k, there):
        total = keep[there]
        for f in range(1, tp):
            pair_copy(k, there, f).wait()
            total = total + pair_recv[there, f].astype(jnp.float32)
        return total

    def line_copy(k, there):
        return remote(
            line_send.at[there], line_recv.at[l], line_ssem.at[k], line_rsem.at[k], line_dev(k)
        )

    order = list(range(1, line)) + [0]
    for i, k in enumerate(order):
        partial(k, lax.rem(l + k, line))
        if i > 0:
            before = order[i - 1]
            there = lax.rem(l + before, line)
            line_send[there] = combine(before, there).astype(jnp.bfloat16)
            line_copy(before, there).start()
    total = after[...] + combine(0, l)
    for k in range(1, line):
        line_copy(k, lax.rem(l + k, line)).wait()
        total = total + line_recv[lax.rem(l + line - k, line)].astype(jnp.float32)
    fin[...] = total.astype(jnp.bfloat16)
    out_ref[t] = fin[...]
    last = [
        remote(fin, out_ref.at[t], fin_ssem.at[f], fin_rsem.at[f], pair_dev(f))
        for f in range(1, tp)
    ]
    for copy in last:
        copy.start()
    for copy in last:
        copy.wait()
    for copy in pending:
        copy.wait_send()


def mixer(
    probe,
    logs,
    key,
    value,
    gate,
    gain,
    out_map,
    residual,
    scale,
    up,
    down,
    line,
    plane,
    outer,
):
    tp = lax.axis_size("tp")
    quads = outer * plane
    sp = quads * line
    positions, width = residual.shape
    share = positions // tp
    rows, hidden = up.shape
    cols = hidden // line
    channels = probe.shape[1]
    heads = channels // HEAD
    tall = channels // sp
    bf16, f32 = jnp.bfloat16, jnp.float32
    dma = pltpu.SemaphoreType.DMA
    return pl.pallas_call(
        functools.partial(mixer_kernel, line, plane, outer, tp),
        out_shape=jax.ShapeDtypeStruct((tp, share, width), bf16),
        in_specs=[pl.BlockSpec(memory_space=pltpu.VMEM)] * 11,
        out_specs=pl.BlockSpec(memory_space=pltpu.VMEM),
        scratch_shapes=[
            pltpu.VMEM((sp, tall + 1, HEAD), f32),
            pltpu.VMEM((positions, channels), f32),
            pltpu.VMEM((positions, channels), f32),
            pltpu.VMEM((heads, HEAD, HEAD), f32),
            pltpu.VMEM((heads, 1, HEAD), f32),
            pltpu.VMEM((sp, tall + 1, HEAD), f32),
            pltpu.VMEM((sp, tall, HEAD), f32),
            pltpu.VMEM((sp, tall, HEAD), f32),
            pltpu.VMEM((tp, share, channels), bf16),
            pltpu.VMEM((tp, share, channels), bf16),
            pltpu.VMEM((tp, channels, width), bf16),
            pltpu.VMEM((share, width), bf16),
            pltpu.VMEM((share, width), f32),
            pltpu.VMEM((sp, rows, cols), bf16),
            pltpu.VMEM((sp, rows, cols), bf16),
            pltpu.VMEM((line, tp, share, width), bf16),
            pltpu.VMEM((line, tp * share, cols), bf16),
            pltpu.VMEM((line, tp, share, width), bf16),
            pltpu.VMEM((line, tp, share, width), bf16),
            pltpu.VMEM((line, share, width), f32),
            pltpu.VMEM((line, share, width), bf16),
            pltpu.VMEM((line, share, width), bf16),
            pltpu.VMEM((share, width), bf16),
            dma((2 * line,)),
            dma((2 * line,)),
            dma((2 * line * quads,)),
            dma((2 * line * quads,)),
            dma((line,)),
            dma((line,)),
            dma((line * tp,)),
            dma((line * tp,)),
            dma((line * tp,)),
            dma((line * tp,)),
            dma((line,)),
            dma((line,)),
            dma((tp,)),
            dma((tp,)),
            dma((sp,)),
            dma((sp,)),
            dma((sp,)),
            dma((sp,)),
            dma((tp,)),
            dma((tp,)),
            dma((tp,)),
            dma((tp,)),
            dma((6,)),
        ],
        compiler_params=pltpu.CompilerParams(
            collective_id=0, has_side_effects=True, vmem_limit_bytes=60 * 1024 * 1024
        ),
    )(
        probe,
        logs,
        key,
        value,
        gate,
        gain.reshape(1, HEAD),
        out_map,
        residual.reshape(tp, share, width),
        scale.reshape(1, width),
        up,
        down,
    )


def body(
    residual_signal,
    reading_probe_preactivations,
    keep_switch_preactivations,
    written_entries,
    emission_switch_preactivations,
    additional_shrink_amount,
    complement_of_floor,
    per_group_rescaler,
    emission_linear_map,
    channel_layer_rescaler,
    expanding_linear_map,
    contracting_linear_map,
):
    logarithmic_keep_fraction = (
        jnp.logaddexp(
            jnp.log1p(-complement_of_floor),
            jnp.log(complement_of_floor)
            + jax.nn.log_sigmoid(keep_switch_preactivations.astype(jnp.float32)),
        )
        + additional_shrink_amount
    )
    key_part = -jnp.expm1(logarithmic_keep_fraction)
    line, plane, outer = grouping(lax.axis_size("sp"))
    finished = mixer(
        reading_probe_preactivations,
        logarithmic_keep_fraction,
        key_part,
        written_entries,
        emission_switch_preactivations,
        per_group_rescaler,
        emission_linear_map,
        residual_signal,
        channel_layer_rescaler,
        expanding_linear_map,
        contracting_linear_map,
        line,
        plane,
        outer,
    )
    return finished.reshape(residual_signal.shape)


def solution(mesh):
    return jax.shard_map(
        body,
        mesh=mesh,
        in_specs=(
            P("sp", None),
            P("sp", "tp"),
            P("sp", "tp"),
            P("sp", "tp"),
            P("sp", "tp"),
            P("sp", "tp"),
            P("tp"),
            P(),
            P("tp", None),
            P(),
            P("sp", "tp"),
            P("sp", "tp"),
        ),
        out_specs=P("sp", None),
        check_vma=False,
    )
```

```python
import functools

import jax
import jax.numpy as jnp
from jax import lax
from jax.experimental import pallas as pl
from jax.experimental.pallas import tpu as pltpu
from jax.sharding import PartitionSpec as P

HEAD = 128
BLOCK = 64


norm_eps = 1e-06
HIGH_ACCURACY = lax.Precision.HIGHEST


MESH = pl.DeviceIdType.MESH
TILE = 256


def grouping(peers):
    line = plane = 4 if peers % 16 == 0 else 1
    return line, plane, peers // (line * plane)


def mixer_kernel(
    line,
    plane,
    outer,
    tp,
    probe_ref,
    logs_ref,
    key_ref,
    value_ref,
    gate_ref,
    gain_ref,
    emission_ref,
    residual_ref,
    scale_ref,
    up_ref,
    down_ref,
    out_ref,
    payload_ref,
    within_ref,
    query_ref,
    state,
    base,
    gathered,
    prefixes,
    prior,
    mixed,
    heads,
    emission,
    normed,
    after,
    up_w,
    down_w,
    tok,
    hid,
    pair_send,
    pair_recv,
    keep,
    line_send,
    line_recv,
    fin,
    s1_send,
    s1_recv,
    s2_send,
    s2_recv,
    tok_send,
    tok_recv,
    tokp_send,
    tokp_recv,
    pair_ssem,
    pair_rsem,
    line_ssem,
    line_rsem,
    fin_ssem,
    fin_rsem,
    state_ssem,
    state_rsem,
    prior_ssem,
    prior_rsem,
    emis_ssem,
    emis_rsem,
    head_ssem,
    head_rsem,
    loc_sem,
):
    quads = outer * plane
    sp = quads * line
    share, width = normed.shape
    rows = up_ref.shape[0]
    cols = up_w.shape[2]
    tall = prefixes.shape[1]
    channels = emission_ref.shape[0]
    local_heads = channels // HEAD
    me, t = lax.axis_index("sp"), lax.axis_index("tp")
    p = lax.rem(me, plane)
    l = lax.rem(me // plane, line)
    o = me // (plane * line)
    q = o * plane + p

    def line_dev(d):
        return ((o * line + lax.rem(l + d, line)) * plane + p, t)

    def quad_dev(e):
        qq = lax.rem(q + e, quads)
        return ((qq // plane * line + l) * plane + lax.rem(qq, plane), t)

    def seq_dev(e):
        return (lax.rem(me + e, sp), t)

    def pair_dev(f):
        return (me, lax.rem(t + f, tp))

    barrier = pltpu.get_barrier_semaphore()
    peers = [seq_dev(e) for e in range(1, sp)] + [pair_dev(f) for f in range(1, tp)]
    for dev in peers:
        pl.semaphore_signal(barrier, inc=1, device_id=dev, device_id_type=MESH)
    pl.semaphore_wait(barrier, len(peers))

    def remote(src, dst, ssem, rsem, dev):
        return pltpu.make_async_remote_copy(
            src_ref=src,
            dst_ref=dst,
            send_sem=ssem,
            recv_sem=rsem,
            device_id=dev,
            device_id_type=MESH,
        )

    pending = []
    mats = ((up_ref, up_w), (down_ref, down_w))

    def first_stage(m):
        src, dst = mats[m]
        copies = []
        for d in range(line):
            there = lax.rem(l + d, line)
            part = src.at[:, pl.ds(pl.multiple_of(there * cols, cols), cols)]
            if d == 0:
                copy = pltpu.make_async_copy(part, dst.at[me], loc_sem.at[m])
            else:
                k = m * line + d
                copy = remote(part, dst.at[me], s1_send.at[k], s1_recv.at[k], line_dev(d))
                pending.append(copy)
            copy.start()
            copies.append(copy)
        return copies

    def second_stage(m, copies):
        dst = mats[m][1]
        for d in range(line):
            if d == 0:
                copies[0].wait()
            else:
                copies[d].wait_recv()
            origin = (o * line + lax.rem(l + line - d, line)) * plane + p
            for e in range(1, quads):
                k = (m * line + d) * quads + e
                copy = remote(
                    dst.at[origin], dst.at[origin], s2_send.at[k], s2_recv.at[k], quad_dev(e)
                )
                copy.start()
                arriving[m].append(copy)

    arriving = ([], [])

    emis_copies = [
        pltpu.make_async_copy(emission_ref, emission.at[t], loc_sem.at[3]),
    ]
    for f in range(1, tp):
        emis_copies.append(
            remote(emission_ref, emission.at[t], emis_ssem.at[f], emis_rsem.at[f], pair_dev(f))
        )
    for copy in emis_copies:
        copy.start()
    up_copies = first_stage(0)
    state[...] = jnp.zeros_like(state)
    base[...] = jnp.zeros_like(base)
    lower = lax.broadcasted_iota(jnp.int32, (BLOCK, BLOCK), 0) >= lax.broadcasted_iota(
        jnp.int32, (BLOCK, BLOCK), 1
    )

    def exact(a, b, ca, cb):
        return lax.dot_general(
            a,
            b,
            (((ca,), (cb,)), ((), ())),
            precision=HIGH_ACCURACY,
            preferred_element_type=jnp.float32,
        )

    @pl.loop(0, probe_ref.shape[0] // BLOCK)
    def _(b):
        at = pl.ds(pl.multiple_of(b * BLOCK, BLOCK), BLOCK)
        sums = exact(lower.astype(jnp.float32), logs_ref[at, :], 1, 0)
        for h in range(local_heads):
            lanes = slice(h * HEAD, (h + 1) * HEAD)
            total = sums[:, lanes]
            end = total[BLOCK - 1 : BLOCK, :]
            middle = 0.5 * end
            query = jax.nn.silu(probe_ref[at, lanes].astype(jnp.float32))
            key = key_ref[at, lanes]
            value = value_ref[at, lanes].astype(jnp.float32)
            scores = exact(query * jnp.exp(total - middle), key * jnp.exp(middle - total), 1, 1)
            scores = jnp.where(lower, scores, 0.0)
            within_ref[at, lanes] = exact(scores, value, 1, 0) + exact(
                query * jnp.exp(total), state[h], 1, 1
            )
            query_ref[at, lanes] = query * jnp.exp(base[h] + total)
            state[h] = jnp.exp(end) * state[h] + exact(value, key * jnp.exp(end - total), 0, 0)
            base[h] = base[h] + end

    each = sp // local_heads
    for k in range(sp):
        h, j = divmod(k, each)
        payload_ref[k, :tall, :] = state[h, j * tall : (j + 1) * tall, :]
        payload_ref[k, tall : tall + 1, :] = jnp.exp(base[h])
    state_copies = []
    for e in range(1, sp):
        there = lax.rem(me + e, sp)
        copy = remote(
            payload_ref.at[there], gathered.at[me], state_ssem.at[e], state_rsem.at[e], seq_dev(e)
        )
        copy.start()
        state_copies.append(copy)
    own = pltpu.make_async_copy(payload_ref.at[me], gathered.at[me], loc_sem.at[2])
    own.start()
    own.wait()
    for copy in state_copies:
        copy.wait()
    run = jnp.zeros((tall, HEAD), jnp.float32)
    for k in range(sp):
        prefixes[k] = run
        run = gathered[k, tall : tall + 1, :] * run + gathered[k, :tall, :]
    prior_copies = []
    for e in range(1, sp):
        there = lax.rem(me + e, sp)
        copy = remote(
            prefixes.at[there], prior.at[me], prior_ssem.at[e], prior_rsem.at[e], seq_dev(e)
        )
        copy.start()
        prior_copies.append(copy)
    prior[me] = prefixes[me]
    down_copies = first_stage(1)
    second_stage(0, up_copies)
    for copy in prior_copies:
        copy.wait()
    before = prior[...].reshape(local_heads, HEAD, HEAD)
    for h in range(local_heads):
        lanes = slice(h * HEAD, (h + 1) * HEAD)
        recur = within_ref[:, lanes] + lax.dot_general(
            query_ref[:, lanes],
            before[h],
            (((1,), (1,)), ((), ())),
            precision=HIGH_ACCURACY,
            preferred_element_type=jnp.float32,
        )
        scaled = (
            recur
            * lax.rsqrt(jnp.mean(recur * recur, axis=-1, keepdims=True) + norm_eps)
            * gain_ref[...]
        )
        gated = scaled * jax.nn.silu(gate_ref[:, lanes].astype(jnp.float32))
        mixed[:, :, lanes] = gated.astype(jnp.bfloat16).reshape(tp, share, HEAD)
    head_copies = [pltpu.make_async_copy(mixed.at[t], heads.at[t], loc_sem.at[4])]
    for f in range(1, tp):
        other = lax.rem(t + f, tp)
        head_copies.append(
            remote(mixed.at[other], heads.at[t], head_ssem.at[f], head_rsem.at[f], pair_dev(f))
        )
    for copy in head_copies:
        copy.start()
    for copy in emis_copies + head_copies:
        copy.wait()
    wide = min(512, width)

    @pl.loop(0, width // wide)
    def _(n):
        at = pl.ds(pl.multiple_of(n * wide, wide), wide)
        value = residual_ref[t, :, at].astype(jnp.float32)
        for c in range(tp):
            value = value + jnp.dot(
                heads[c], emission[c, :, at], preferred_element_type=jnp.float32
            )
        after[:, at] = value

    square = jnp.mean(after[...] * after[...], axis=-1, keepdims=True)
    normed[...] = (after[...] * lax.rsqrt(square + norm_eps) * scale_ref[...]).astype(
        jnp.bfloat16
    )
    own = pltpu.make_async_copy(normed, tok.at[l, t], loc_sem.at[5])
    own.start()
    token_copies = [own]
    for d in range(1, line):
        copy = remote(normed, tok.at[l, t], tok_send.at[d], tok_recv.at[d], line_dev(d))
        copy.start()
        pending.append(copy)
        token_copies.append(copy)
    second_stage(1, down_copies)
    for copy in arriving[0]:
        copy.wait()
    tile = min(TILE, cols)

    def receive(d):
        origin = lax.rem(l + line - d, line)
        if d == 0:
            own.wait()
        else:
            token_copies[d].wait_recv()
        copies = []
        for f in range(1, tp):
            k = d * tp + f
            copy = remote(
                tok.at[origin, t], tok.at[origin, t], tokp_send.at[k], tokp_recv.at[k], pair_dev(f)
            )
            copy.start()
            copies.append(copy)
        for copy in copies:
            copy.wait()

    def expand(block):
        @pl.loop(0, cols // tile)
        def _(n):
            at = pl.ds(pl.multiple_of(n * tile, tile), tile)
            value = jnp.dot(
                tok[block].reshape(tp * share, width),
                up_w[:, :, at].reshape(width, tile),
                preferred_element_type=jnp.float32,
            )
            value = jnp.maximum(value, 0.0)
            hid[block, :, at] = (value * value).astype(jnp.bfloat16)

    def pair_copy(k, there, f):
        other = lax.rem(t + f, tp)
        i = k * tp + f
        return remote(
            pair_send.at[there, other],
            pair_recv.at[there, f],
            pair_ssem.at[i],
            pair_rsem.at[i],
            pair_dev(f),
        )

    group = width // (line * rows)
    assert group == quads

    def partial(k, there):
        @pl.loop(0, quads)
        def _(n):
            at = pl.ds(pl.multiple_of(n * line * rows, line * rows), line * rows)
            value = lax.dot_general(
                hid[there],
                down_w[pl.ds(n * line, line)].reshape(line * rows, cols),
                (((1,), (1,)), ((), ())),
                preferred_element_type=jnp.float32,
            ).reshape(tp, share, line * rows)
            pair_send[there, :, :, at] = value.astype(jnp.bfloat16)
            for c in range(tp):

                @pl.when(t == c)
                def _():
                    keep[there, :, at] = value[c]

        for f in range(1, tp):
            pair_copy(k, there, f).start()

    def combine(k, there):
        total = keep[there]
        for f in range(1, tp):
            pair_copy(k, there, f).wait()
            total = total + pair_recv[there, f].astype(jnp.float32)
        return total

    def line_copy(k, there):
        return remote(
            line_send.at[there], line_recv.at[l], line_ssem.at[k], line_rsem.at[k], line_dev(k)
        )

    def send_line(k):
        there = lax.rem(l + k, line)
        line_send[there] = combine(k, there).astype(jnp.bfloat16)
        line_copy(k, there).start()

    for d in range(line):
        k = (line - d) % line
        there = lax.rem(l + k, line)
        receive(d)
        expand(there)
        if d == 0:
            for copy in arriving[1]:
                copy.wait()
        partial(k, there)
        if k:
            send_line(k)
    total = after[...] + combine(0, l)
    for k in range(1, line):
        line_copy(k, lax.rem(l + k, line)).wait()
        total = total + line_recv[lax.rem(l + line - k, line)].astype(jnp.float32)
    fin[...] = total.astype(jnp.bfloat16)
    out_ref[t] = fin[...]
    last = [
        remote(fin, out_ref.at[t], fin_ssem.at[f], fin_rsem.at[f], pair_dev(f))
        for f in range(1, tp)
    ]
    for copy in last:
        copy.start()
    for copy in last:
        copy.wait()
    for copy in pending:
        copy.wait_send()


def mixer(
    probe,
    logs,
    key,
    value,
    gate,
    gain,
    out_map,
    residual,
    scale,
    up,
    down,
    line,
    plane,
    outer,
):
    tp = lax.axis_size("tp")
    quads = outer * plane
    sp = quads * line
    positions, width = residual.shape
    share = positions // tp
    rows, hidden = up.shape
    cols = hidden // line
    channels = probe.shape[1]
    heads = channels // HEAD
    tall = channels // sp
    bf16, f32 = jnp.bfloat16, jnp.float32
    dma = pltpu.SemaphoreType.DMA
    return pl.pallas_call(
        functools.partial(mixer_kernel, line, plane, outer, tp),
        out_shape=jax.ShapeDtypeStruct((tp, share, width), bf16),
        in_specs=[pl.BlockSpec(memory_space=pltpu.VMEM)] * 11,
        out_specs=pl.BlockSpec(memory_space=pltpu.VMEM),
        scratch_shapes=[
            pltpu.VMEM((sp, tall + 1, HEAD), f32),
            pltpu.VMEM((positions, channels), f32),
            pltpu.VMEM((positions, channels), f32),
            pltpu.VMEM((heads, HEAD, HEAD), f32),
            pltpu.VMEM((heads, 1, HEAD), f32),
            pltpu.VMEM((sp, tall + 1, HEAD), f32),
            pltpu.VMEM((sp, tall, HEAD), f32),
            pltpu.VMEM((sp, tall, HEAD), f32),
            pltpu.VMEM((tp, share, channels), bf16),
            pltpu.VMEM((tp, share, channels), bf16),
            pltpu.VMEM((tp, channels, width), bf16),
            pltpu.VMEM((share, width), bf16),
            pltpu.VMEM((share, width), f32),
            pltpu.VMEM((sp, rows, cols), bf16),
            pltpu.VMEM((sp, rows, cols), bf16),
            pltpu.VMEM((line, tp, share, width), bf16),
            pltpu.VMEM((line, tp * share, cols), bf16),
            pltpu.VMEM((line, tp, share, width), bf16),
            pltpu.VMEM((line, tp, share, width), bf16),
            pltpu.VMEM((line, share, width), f32),
            pltpu.VMEM((line, share, width), bf16),
            pltpu.VMEM((line, share, width), bf16),
            pltpu.VMEM((share, width), bf16),
            dma((2 * line,)),
            dma((2 * line,)),
            dma((2 * line * quads,)),
            dma((2 * line * quads,)),
            dma((line,)),
            dma((line,)),
            dma((line * tp,)),
            dma((line * tp,)),
            dma((line * tp,)),
            dma((line * tp,)),
            dma((line,)),
            dma((line,)),
            dma((tp,)),
            dma((tp,)),
            dma((sp,)),
            dma((sp,)),
            dma((sp,)),
            dma((sp,)),
            dma((tp,)),
            dma((tp,)),
            dma((tp,)),
            dma((tp,)),
            dma((6,)),
        ],
        compiler_params=pltpu.CompilerParams(
            collective_id=0, has_side_effects=True, vmem_limit_bytes=60 * 1024 * 1024
        ),
    )(
        probe,
        logs,
        key,
        value,
        gate,
        gain.reshape(1, HEAD),
        out_map,
        residual.reshape(tp, share, width),
        scale.reshape(1, width),
        up,
        down,
    )


def body(
    residual_signal,
    reading_probe_preactivations,
    keep_switch_preactivations,
    written_entries,
    emission_switch_preactivations,
    additional_shrink_amount,
    complement_of_floor,
    per_group_rescaler,
    emission_linear_map,
    channel_layer_rescaler,
    expanding_linear_map,
    contracting_linear_map,
):
    logarithmic_keep_fraction = (
        jnp.logaddexp(
            jnp.log1p(-complement_of_floor),
            jnp.log(complement_of_floor)
            + jax.nn.log_sigmoid(keep_switch_preactivations.astype(jnp.float32)),
        )
        + additional_shrink_amount
    )
    key_part = -jnp.expm1(logarithmic_keep_fraction)
    line, plane, outer = grouping(lax.axis_size("sp"))
    finished = mixer(
        reading_probe_preactivations,
        logarithmic_keep_fraction,
        key_part,
        written_entries,
        emission_switch_preactivations,
        per_group_rescaler,
        emission_linear_map,
        residual_signal,
        channel_layer_rescaler,
        expanding_linear_map,
        contracting_linear_map,
        line,
        plane,
        outer,
    )
    return finished.reshape(residual_signal.shape)


def solution(mesh):
    return jax.shard_map(
        body,
        mesh=mesh,
        in_specs=(
            P("sp", None),
            P("sp", "tp"),
            P("sp", "tp"),
            P("sp", "tp"),
            P("sp", "tp"),
            P("sp", "tp"),
            P("tp"),
            P(),
            P("tp", None),
            P(),
            P("sp", "tp"),
            P("sp", "tp"),
        ),
        out_specs=P("sp", None),
        check_vma=False,
    )
```

```python
import functools

import jax
import jax.numpy as jnp
from jax import lax
from jax.experimental import pallas as pl
from jax.experimental.pallas import tpu as pltpu
from jax.sharding import PartitionSpec as P

HEAD = 128
BLOCK = 64


norm_eps = 1e-06
HIGH_ACCURACY = lax.Precision.HIGHEST


MESH = pl.DeviceIdType.MESH
TILE = 256


def grouping(peers):
    line = plane = 4 if peers % 16 == 0 else 1
    return line, plane, peers // (line * plane)


def mixer_kernel(
    line,
    plane,
    outer,
    tp,
    probe_ref,
    logs_ref,
    key_ref,
    value_ref,
    gate_ref,
    gain_ref,
    emission_ref,
    residual_ref,
    scale_ref,
    up_ref,
    down_ref,
    out_ref,
    payload_ref,
    within_ref,
    query_ref,
    state,
    base,
    gathered,
    prefixes,
    prior,
    mixed,
    heads,
    emission,
    normed,
    after,
    up_w,
    down_w,
    tok,
    hid,
    pair_send,
    pair_recv,
    keep,
    line_send,
    line_recv,
    fin,
    s1_send,
    s1_recv,
    s2_send,
    s2_recv,
    tok_send,
    tok_recv,
    tokp_send,
    tokp_recv,
    pair_ssem,
    pair_rsem,
    line_ssem,
    line_rsem,
    fin_ssem,
    fin_rsem,
    state_ssem,
    state_rsem,
    prior_ssem,
    prior_rsem,
    emis_ssem,
    emis_rsem,
    head_ssem,
    head_rsem,
    loc_sem,
):
    quads = outer * plane
    sp = quads * line
    share, width = normed.shape
    rows = up_ref.shape[0]
    cols = up_w.shape[2]
    tall = prefixes.shape[1]
    channels = emission_ref.shape[0]
    local_heads = channels // HEAD
    me, t = lax.axis_index("sp"), lax.axis_index("tp")
    p = lax.rem(me, plane)
    l = lax.rem(me // plane, line)
    o = me // (plane * line)
    q = o * plane + p

    def line_dev(d):
        return ((o * line + lax.rem(l + d, line)) * plane + p, t)

    def quad_dev(e):
        qq = lax.rem(q + e, quads)
        return ((qq // plane * line + l) * plane + lax.rem(qq, plane), t)

    def seq_dev(e):
        return (lax.rem(me + e, sp), t)

    def pair_dev(f):
        return (me, lax.rem(t + f, tp))

    barrier = pltpu.get_barrier_semaphore()
    peers = [seq_dev(e) for e in range(1, sp)] + [pair_dev(f) for f in range(1, tp)]
    for dev in peers:
        pl.semaphore_signal(barrier, inc=1, device_id=dev, device_id_type=MESH)
    pl.semaphore_wait(barrier, len(peers))

    def remote(src, dst, ssem, rsem, dev):
        return pltpu.make_async_remote_copy(
            src_ref=src,
            dst_ref=dst,
            send_sem=ssem,
            recv_sem=rsem,
            device_id=dev,
            device_id_type=MESH,
        )

    pending = []
    mats = ((up_ref, up_w), (down_ref, down_w))

    def first_stage(m):
        src, dst = mats[m]
        copies = []
        for d in range(line):
            there = lax.rem(l + d, line)
            part = src.at[:, pl.ds(pl.multiple_of(there * cols, cols), cols)]
            if d == 0:
                copy = pltpu.make_async_copy(part, dst.at[me], loc_sem.at[m])
            else:
                k = m * line + d
                copy = remote(part, dst.at[me], s1_send.at[k], s1_recv.at[k], line_dev(d))
                pending.append(copy)
            copy.start()
            copies.append(copy)
        return copies

    def second_stage(m, copies, steps):
        dst = mats[m][1]
        for d in steps:
            if d == 0:
                copies[0].wait()
            else:
                copies[d].wait_recv()
            origin = (o * line + lax.rem(l + line - d, line)) * plane + p
            for e in range(1, quads):
                k = (m * line + d) * quads + e
                copy = remote(
                    dst.at[origin], dst.at[origin], s2_send.at[k], s2_recv.at[k], quad_dev(e)
                )
                copy.start()
                arriving[m].append(copy)

    arriving = ([], [])

    emis_copies = [
        pltpu.make_async_copy(emission_ref, emission.at[t], loc_sem.at[3]),
    ]
    for f in range(1, tp):
        emis_copies.append(
            remote(emission_ref, emission.at[t], emis_ssem.at[f], emis_rsem.at[f], pair_dev(f))
        )
    for copy in emis_copies:
        copy.start()
    up_copies = first_stage(0)
    second_stage(0, up_copies, range(1))
    state[...] = jnp.zeros_like(state)
    base[...] = jnp.zeros_like(base)
    lower = lax.broadcasted_iota(jnp.int32, (BLOCK, BLOCK), 0) >= lax.broadcasted_iota(
        jnp.int32, (BLOCK, BLOCK), 1
    )

    def exact(a, b, ca, cb):
        return lax.dot_general(
            a,
            b,
            (((ca,), (cb,)), ((), ())),
            precision=HIGH_ACCURACY,
            preferred_element_type=jnp.float32,
        )

    @pl.loop(0, probe_ref.shape[0] // BLOCK)
    def _(b):
        at = pl.ds(pl.multiple_of(b * BLOCK, BLOCK), BLOCK)
        sums = exact(lower.astype(jnp.float32), logs_ref[at, :], 1, 0)
        for h in range(local_heads):
            lanes = slice(h * HEAD, (h + 1) * HEAD)
            total = sums[:, lanes]
            end = total[BLOCK - 1 : BLOCK, :]
            middle = 0.5 * end
            query = jax.nn.silu(probe_ref[at, lanes].astype(jnp.float32))
            key = key_ref[at, lanes]
            value = value_ref[at, lanes].astype(jnp.float32)
            scores = exact(query * jnp.exp(total - middle), key * jnp.exp(middle - total), 1, 1)
            scores = jnp.where(lower, scores, 0.0)
            within_ref[at, lanes] = exact(scores, value, 1, 0) + exact(
                query * jnp.exp(total), state[h], 1, 1
            )
            query_ref[at, lanes] = query * jnp.exp(base[h] + total)
            state[h] = jnp.exp(end) * state[h] + exact(value, key * jnp.exp(end - total), 0, 0)
            base[h] = base[h] + end

    each = sp // local_heads
    for k in range(sp):
        h, j = divmod(k, each)
        payload_ref[k, :tall, :] = state[h, j * tall : (j + 1) * tall, :]
        payload_ref[k, tall : tall + 1, :] = jnp.exp(base[h])
    state_copies = []
    for e in range(1, sp):
        there = lax.rem(me + e, sp)
        copy = remote(
            payload_ref.at[there], gathered.at[me], state_ssem.at[e], state_rsem.at[e], seq_dev(e)
        )
        copy.start()
        state_copies.append(copy)
    own = pltpu.make_async_copy(payload_ref.at[me], gathered.at[me], loc_sem.at[2])
    own.start()
    second_stage(0, up_copies, range(1, line))
    own.wait()
    for copy in state_copies:
        copy.wait()
    run = jnp.zeros((tall, HEAD), jnp.float32)
    for k in range(sp):
        prefixes[k] = run
        run = gathered[k, tall : tall + 1, :] * run + gathered[k, :tall, :]
    prior_copies = []
    for e in range(1, sp):
        there = lax.rem(me + e, sp)
        copy = remote(
            prefixes.at[there], prior.at[me], prior_ssem.at[e], prior_rsem.at[e], seq_dev(e)
        )
        copy.start()
        prior_copies.append(copy)
    prior[me] = prefixes[me]
    down_copies = first_stage(1)
    second_stage(1, down_copies, range(1))
    for copy in prior_copies:
        copy.wait()
    before = prior[...].reshape(local_heads, HEAD, HEAD)
    for h in range(local_heads):
        lanes = slice(h * HEAD, (h + 1) * HEAD)
        recur = within_ref[:, lanes] + lax.dot_general(
            query_ref[:, lanes],
            before[h],
            (((1,), (1,)), ((), ())),
            precision=HIGH_ACCURACY,
            preferred_element_type=jnp.float32,
        )
        scaled = (
            recur
            * lax.rsqrt(jnp.mean(recur * recur, axis=-1, keepdims=True) + norm_eps)
            * gain_ref[...]
        )
        gated = scaled * jax.nn.silu(gate_ref[:, lanes].astype(jnp.float32))
        mixed[:, :, lanes] = gated.astype(jnp.bfloat16).reshape(tp, share, HEAD)
    head_copies = [pltpu.make_async_copy(mixed.at[t], heads.at[t], loc_sem.at[4])]
    for f in range(1, tp):
        other = lax.rem(t + f, tp)
        head_copies.append(
            remote(mixed.at[other], heads.at[t], head_ssem.at[f], head_rsem.at[f], pair_dev(f))
        )
    for copy in head_copies:
        copy.start()
    for copy in emis_copies + head_copies:
        copy.wait()
    wide = min(512, width)

    @pl.loop(0, width // wide)
    def _(n):
        at = pl.ds(pl.multiple_of(n * wide, wide), wide)
        value = residual_ref[t, :, at].astype(jnp.float32)
        for c in range(tp):
            value = value + jnp.dot(
                heads[c], emission[c, :, at], preferred_element_type=jnp.float32
            )
        after[:, at] = value

    square = jnp.mean(after[...] * after[...], axis=-1, keepdims=True)
    normed[...] = (after[...] * lax.rsqrt(square + norm_eps) * scale_ref[...]).astype(
        jnp.bfloat16
    )
    own = pltpu.make_async_copy(normed, tok.at[l, t], loc_sem.at[5])
    own.start()
    token_copies = [own]
    for d in range(1, line):
        copy = remote(normed, tok.at[l, t], tok_send.at[d], tok_recv.at[d], line_dev(d))
        copy.start()
        pending.append(copy)
        token_copies.append(copy)
    second_stage(1, down_copies, range(1, line))
    pair_tokens = []
    for d in range(line):
        if d == 0:
            own.wait()
        else:
            token_copies[d].wait_recv()
        origin = lax.rem(l + line - d, line)
        for f in range(1, tp):
            k = d * tp + f
            copy = remote(
                tok.at[origin, t], tok.at[origin, t], tokp_send.at[k], tokp_recv.at[k], pair_dev(f)
            )
            copy.start()
            pair_tokens.append(copy)
    for copy in arriving[0]:
        copy.wait()
    for copy in pair_tokens:
        copy.wait()

    tile = min(TILE, cols)
    for block in range(line):

        @pl.loop(0, cols // tile)
        def _(n):
            at = pl.ds(pl.multiple_of(n * tile, tile), tile)
            value = jnp.dot(
                tok[block].reshape(tp * share, width),
                up_w[:, :, at].reshape(width, tile),
                preferred_element_type=jnp.float32,
            )
            value = jnp.maximum(value, 0.0)
            hid[block, :, at] = (value * value).astype(jnp.bfloat16)

    for copy in arriving[1]:
        copy.wait()

    def pair_copy(k, there, f):
        other = lax.rem(t + f, tp)
        i = k * tp + f
        return remote(
            pair_send.at[there, other],
            pair_recv.at[there, f],
            pair_ssem.at[i],
            pair_rsem.at[i],
            pair_dev(f),
        )

    group = width // (line * rows)
    assert group == quads

    def partial(k, there):
        @pl.loop(0, quads)
        def _(n):
            at = pl.ds(pl.multiple_of(n * line * rows, line * rows), line * rows)
            value = lax.dot_general(
                hid[there],
                down_w[pl.ds(n * line, line)].reshape(line * rows, cols),
                (((1,), (1,)), ((), ())),
                preferred_element_type=jnp.float32,
            ).reshape(tp, share, line * rows)
            pair_send[there, :, :, at] = value.astype(jnp.bfloat16)
            for c in range(tp):

                @pl.when(t == c)
                def _():
                    keep[there, :, at] = value[c]

        for f in range(1, tp):
            pair_copy(k, there, f).start()

    def combine(k, there):
        total = keep[there]
        for f in range(1, tp):
            pair_copy(k, there, f).wait()
            total = total + pair_recv[there, f].astype(jnp.float32)
        return total

    def line_copy(k, there):
        return remote(
            line_send.at[there], line_recv.at[l], line_ssem.at[k], line_rsem.at[k], line_dev(k)
        )

    order = list(range(1, line)) + [0]
    for i, k in enumerate(order):
        partial(k, lax.rem(l + k, line))
        if i > 0:
            before = order[i - 1]
            there = lax.rem(l + before, line)
            line_send[there] = combine(before, there).astype(jnp.bfloat16)
            line_copy(before, there).start()
    total = after[...] + combine(0, l)
    for k in range(1, line):
        line_copy(k, lax.rem(l + k, line)).wait()
        total = total + line_recv[lax.rem(l + line - k, line)].astype(jnp.float32)
    fin[...] = total.astype(jnp.bfloat16)
    out_ref[t] = fin[...]
    last = [
        remote(fin, out_ref.at[t], fin_ssem.at[f], fin_rsem.at[f], pair_dev(f))
        for f in range(1, tp)
    ]
    for copy in last:
        copy.start()
    for copy in last:
        copy.wait()
    for copy in pending:
        copy.wait_send()


def mixer(
    probe,
    logs,
    key,
    value,
    gate,
    gain,
    out_map,
    residual,
    scale,
    up,
    down,
    line,
    plane,
    outer,
):
    tp = lax.axis_size("tp")
    quads = outer * plane
    sp = quads * line
    positions, width = residual.shape
    share = positions // tp
    rows, hidden = up.shape
    cols = hidden // line
    channels = probe.shape[1]
    heads = channels // HEAD
    tall = channels // sp
    bf16, f32 = jnp.bfloat16, jnp.float32
    dma = pltpu.SemaphoreType.DMA
    return pl.pallas_call(
        functools.partial(mixer_kernel, line, plane, outer, tp),
        out_shape=jax.ShapeDtypeStruct((tp, share, width), bf16),
        in_specs=[pl.BlockSpec(memory_space=pltpu.VMEM)] * 11,
        out_specs=pl.BlockSpec(memory_space=pltpu.VMEM),
        scratch_shapes=[
            pltpu.VMEM((sp, tall + 1, HEAD), f32),
            pltpu.VMEM((positions, channels), f32),
            pltpu.VMEM((positions, channels), f32),
            pltpu.VMEM((heads, HEAD, HEAD), f32),
            pltpu.VMEM((heads, 1, HEAD), f32),
            pltpu.VMEM((sp, tall + 1, HEAD), f32),
            pltpu.VMEM((sp, tall, HEAD), f32),
            pltpu.VMEM((sp, tall, HEAD), f32),
            pltpu.VMEM((tp, share, channels), bf16),
            pltpu.VMEM((tp, share, channels), bf16),
            pltpu.VMEM((tp, channels, width), bf16),
            pltpu.VMEM((share, width), bf16),
            pltpu.VMEM((share, width), f32),
            pltpu.VMEM((sp, rows, cols), bf16),
            pltpu.VMEM((sp, rows, cols), bf16),
            pltpu.VMEM((line, tp, share, width), bf16),
            pltpu.VMEM((line, tp * share, cols), bf16),
            pltpu.VMEM((line, tp, share, width), bf16),
            pltpu.VMEM((line, tp, share, width), bf16),
            pltpu.VMEM((line, share, width), f32),
            pltpu.VMEM((line, share, width), bf16),
            pltpu.VMEM((line, share, width), bf16),
            pltpu.VMEM((share, width), bf16),
            dma((2 * line,)),
            dma((2 * line,)),
            dma((2 * line * quads,)),
            dma((2 * line * quads,)),
            dma((line,)),
            dma((line,)),
            dma((line * tp,)),
            dma((line * tp,)),
            dma((line * tp,)),
            dma((line * tp,)),
            dma((line,)),
            dma((line,)),
            dma((tp,)),
            dma((tp,)),
            dma((sp,)),
            dma((sp,)),
            dma((sp,)),
            dma((sp,)),
            dma((tp,)),
            dma((tp,)),
            dma((tp,)),
            dma((tp,)),
            dma((6,)),
        ],
        compiler_params=pltpu.CompilerParams(
            collective_id=0, has_side_effects=True, vmem_limit_bytes=60 * 1024 * 1024
        ),
    )(
        probe,
        logs,
        key,
        value,
        gate,
        gain.reshape(1, HEAD),
        out_map,
        residual.reshape(tp, share, width),
        scale.reshape(1, width),
        up,
        down,
    )


def body(
    residual_signal,
    reading_probe_preactivations,
    keep_switch_preactivations,
    written_entries,
    emission_switch_preactivations,
    additional_shrink_amount,
    complement_of_floor,
    per_group_rescaler,
    emission_linear_map,
    channel_layer_rescaler,
    expanding_linear_map,
    contracting_linear_map,
):
    logarithmic_keep_fraction = (
        jnp.logaddexp(
            jnp.log1p(-complement_of_floor),
            jnp.log(complement_of_floor)
            + jax.nn.log_sigmoid(keep_switch_preactivations.astype(jnp.float32)),
        )
        + additional_shrink_amount
    )
    key_part = -jnp.expm1(logarithmic_keep_fraction)
    line, plane, outer = grouping(lax.axis_size("sp"))
    finished = mixer(
        reading_probe_preactivations,
        logarithmic_keep_fraction,
        key_part,
        written_entries,
        emission_switch_preactivations,
        per_group_rescaler,
        emission_linear_map,
        residual_signal,
        channel_layer_rescaler,
        expanding_linear_map,
        contracting_linear_map,
        line,
        plane,
        outer,
    )
    return finished.reshape(residual_signal.shape)


def solution(mesh):
    return jax.shard_map(
        body,
        mesh=mesh,
        in_specs=(
            P("sp", None),
            P("sp", "tp"),
            P("sp", "tp"),
            P("sp", "tp"),
            P("sp", "tp"),
            P("sp", "tp"),
            P("tp"),
            P(),
            P("tp", None),
            P(),
            P("sp", "tp"),
            P("sp", "tp"),
        ),
        out_specs=P("sp", None),
        check_vma=False,
    )
```
